32 devices in a mesh: pp: 4 (over z), fs: 2 (over y), tp: 4 (over x, core).
Axes of the slice: x: 2, y: 2, z: 4, core: 2. Of those that a mesh axis runs over, the one named last changes fastest.
Arguments:
- tokens_in: bfloat16 [4, 8, 8, 2048], P('pp', ('fs', 'tp')), may hold values from -6 to 6
- weight_in: bfloat16 [4, 2048, 512], P('pp'), may hold values from -0.125 to 0.125
- conv_taps: float32 [4, 4, 512], P('pp'), may hold values from -3 to 3
- conv_bias: float32 [4, 512], P('pp'), may hold values from -2 to 2
- gate_rate: bfloat16 [4, 8, 64, 64], P('pp'), may hold values from -0.75 to 0.75
- bias_rate: float32 [4, 512], P('pp'), may hold values from -3 to 3
- gate_input: bfloat16 [4, 8, 64, 64], P('pp'), may hold values from -0.75 to 0.75
- bias_input: float32 [4, 512], P('pp'), may hold values from -3 to 3
- decay_param: float32 [4, 512], P('pp'), may hold values from 3.5 to 7.5
- weight_out: bfloat16 [4, 512, 2048], P('pp'), may hold values from -0.5 to 0.5
- norm_gain: float32 [4, 2048], P('pp'), may hold values from 0.1 to 1.9
- norm_shift: float32 [4, 2048], P('pp'), may hold values from -2 to 2
Outputs:
- tokens_out: bfloat16 [4, 8, 8, 2048], P('pp', ('fs', 'tp'))
The draws below stay inside these ranges and needn't reach their ends.
All inputs are finite; a program needn't handle non-finite values.
Results may differ from the reference program's by a relative error of at most 0.022.
Values may be sent and summed in bfloat16 or wider, within the bound.
A program may use at most 128 MiB of HBM per device.

```python
import jax
import jax.numpy as jnp
from jax import lax

D = 2048
LRU_W = 512
LRU_BLOCKS = 8
BLOCK_W = 64
CONV = 4
LEN = 8
SECTIONS = 4
SEQS = 8


def shard_levels(stream_key, shape, pieces, least, largest):
    def one(axis_at, shards_of):
        draws = jax.random.uniform(jax.random.fold_in(jax.random.fold_in(stream_key, 6), axis_at), (shards_of,), jnp.float32, least / len(pieces), largest / len(pieces))
        return jnp.repeat(jnp.exp(draws), shape[axis_at] // shards_of).reshape((-1,) + (1,) * (len(shape) - axis_at - 1))

    gain = one(*pieces[0])
    for cut in pieces[1:]:
        gain = gain * one(*cut)
    return gain


def centred(stream_key, shape, spread, bound, pieces=(), kind=jnp.bfloat16):
    factor_of = shard_levels(stream_key, shape, pieces, -0.22, 0.18) if pieces else 1.0
    entries = jax.random.normal(stream_key, shape, jnp.float32) * spread * factor_of
    return jnp.minimum(jnp.maximum(entries, -bound), bound).astype(kind)


def setup_inputs(seed: int = 0) -> dict:
    streams_of = jax.random.split(jax.random.key(seed), 13)
    tokens_in = centred(streams_of[0], (SECTIONS, SEQS, LEN, D), 1.0, 6.0, ((0, 4), (1, 8)))
    weight_in = centred(streams_of[1], (SECTIONS, D, LRU_W), D ** -0.5, 0.125, ((0, 4),))
    conv_taps = centred(streams_of[2], (SECTIONS, CONV, LRU_W), 0.5, 3.0, ((0, 4),), jnp.float32)
    conv_bias = centred(streams_of[3], (SECTIONS, LRU_W), 0.3, 2.0, ((0, 4),), jnp.float32)
    gate_rate = centred(streams_of[4], (SECTIONS, LRU_BLOCKS, BLOCK_W, BLOCK_W), BLOCK_W ** -0.5, 0.75, ((0, 4),))
    bias_rate = centred(streams_of[5], (SECTIONS, LRU_W), 0.5, 3.0, ((0, 4),), jnp.float32)
    gate_input = centred(streams_of[6], (SECTIONS, LRU_BLOCKS, BLOCK_W, BLOCK_W), BLOCK_W ** -0.5, 0.75, ((0, 4),))
    bias_input = centred(streams_of[7], (SECTIONS, LRU_W), 0.5, 3.0, ((0, 4),), jnp.float32)
    decay_param = jnp.clip(3.5 + 4.0 * jax.random.uniform(streams_of[8], (SECTIONS, LRU_W), jnp.float32) ** shard_levels(streams_of[8], (SECTIONS, LRU_W), ((0, 4),), -0.2, 0.2), 3.5, 7.5)
    weight_out = centred(streams_of[9], (SECTIONS, LRU_W, D), (LRU_W // 4) ** -0.5, 0.5, ((0, 4),))
    norm_gain = jnp.clip(1.0 + 0.18 * jax.random.normal(streams_of[10], (SECTIONS, D), jnp.float32), 0.1, 1.9)
    norm_shift = centred(streams_of[11], (SECTIONS, D), 0.3, 2.0, ((0, 4),), jnp.float32)
    return dict(tokens_in=tokens_in, weight_in=weight_in, conv_taps=conv_taps, conv_bias=conv_bias, gate_rate=gate_rate, bias_rate=bias_rate, gate_input=gate_input, bias_input=bias_input, decay_param=decay_param, weight_out=weight_out, norm_gain=norm_gain, norm_shift=norm_shift)


decay_scale = 8.0
norm_eps = 1e-05

def combine_steps(earlier, later):
    return (earlier[0] * later[0], later[0] * earlier[1] + later[1])

def recurrence(projected, conv_taps, conv_bias, gate_rate, bias_rate, gate_input, bias_input, decay_param):
    seq_count, length, channels = projected.shape
    tap_count = conv_taps.shape[0]
    padded = jnp.pad(projected.astype(jnp.float32), ((0, 0), (tap_count - 1, 0), (0, 0)))
    convolved = conv_bias + padded[:, 0:length] * conv_taps[0]
    for tap_index in range(1, tap_count):
        convolved = convolved + padded[:, tap_index:tap_index + length] * conv_taps[tap_index]
    convolved = convolved.astype(jnp.bfloat16)
    blocks = gate_rate.shape[0]
    block_width = gate_rate.shape[1]
    grouped = convolved.astype(jnp.float32).reshape(seq_count, length, blocks, block_width)
    rate_pre = jnp.einsum('bsnc,ncd->bsnd', grouped, gate_rate.astype(jnp.float32))
    input_pre = jnp.einsum('bsnc,ncd->bsnd', grouped, gate_input.astype(jnp.float32))
    rate_gate = jax.nn.sigmoid(rate_pre.reshape(seq_count, length, channels) + bias_rate)
    input_gate = jax.nn.sigmoid(input_pre.reshape(seq_count, length, channels) + bias_input)
    log_decay = -decay_scale * rate_gate * jax.nn.softplus(-decay_param)
    scale_in = jnp.sqrt(-jnp.expm1(2.0 * log_decay))
    driven = scale_in * input_gate * convolved.astype(jnp.float32)
    decay_now = jnp.exp(log_decay)
    unused, hidden = lax.associative_scan(combine_steps, (decay_now, driven), axis=1)
    return hidden.astype(jnp.bfloat16)

def finish(stream_rows, mixed_rows, weight_out, norm_gain, norm_shift):
    summed = stream_rows.astype(jnp.float32) + jnp.dot(mixed_rows, weight_out, preferred_element_type=jnp.float32)
    mean_value = lax.optimization_barrier(jnp.mean(summed, axis=-1, keepdims=True))
    centered = summed - mean_value
    variance = lax.optimization_barrier(jnp.mean(centered * centered, axis=-1, keepdims=True))
    return (centered * lax.rsqrt(variance + norm_eps) * norm_gain + norm_shift).astype(jnp.bfloat16)

def reference(tokens_in, weight_in, conv_taps, conv_bias, gate_rate, bias_rate, gate_input, bias_input, decay_param, weight_out, norm_gain, norm_shift):
    length = tokens_in.shape[2]
    model_width = tokens_in.shape[3]
    stream = tokens_in.reshape(-1, length, model_width)
    seq_count = stream.shape[0]

    def apply_section(current, section_weights):
        w_project, taps_now, cbias_now, grate_now, brate_now, ginput_now, binput_now, dparam_now, w_back, gain_now, shift_now = section_weights
        lru_width = w_project.shape[1]
        flat_rows = current.reshape(seq_count * length, model_width)
        projected = jnp.dot(flat_rows, w_project, preferred_element_type=jnp.float32).astype(jnp.bfloat16)
        projected = projected.reshape(seq_count, length, lru_width)
        mixed_out = recurrence(projected, taps_now, cbias_now, grate_now, brate_now, ginput_now, binput_now, dparam_now)
        result = finish(flat_rows, mixed_out.reshape(seq_count * length, lru_width), w_back, gain_now, shift_now)
        return (result.reshape(seq_count, length, model_width), None)
    stream, unused = lax.scan(apply_section, stream, (weight_in, conv_taps, conv_bias, gate_rate, bias_rate, gate_input, bias_input, decay_param, weight_out, norm_gain, norm_shift))
    return stream.reshape(tokens_in.shape)
```

```python
import functools

import jax
import jax.numpy as jnp
from jax import lax
from jax.experimental import pallas as pl
from jax.experimental.pallas import tpu as pltpu
from jax.sharding import PartitionSpec as P

decay_scale = 8.0
norm_eps = 1e-05
mxu_width = 256
stream_parts = 4
MESH = pl.DeviceIdType.MESH


def stack_kernel(
    sections,
    tokens_hbm,
    w_in_hbm,
    taps_hbm,
    cbias_hbm,
    grate_hbm,
    brate_hbm,
    ginput_hbm,
    binput_hbm,
    dparam_hbm,
    w_out_hbm,
    gain_hbm,
    shift_hbm,
    out_ref,
    w_in,
    w_out,
    taps,
    cbias,
    grate,
    brate,
    ginput,
    binput,
    dparam,
    gain,
    shift,
    rate_map,
    input_map,
    mine,
    inbox,
    outbox,
    load_sem,
    entry_sem,
    send_sem,
    recv_sem,
    final_sem,
    ready_sem,
):
    section = lax.axis_index("pp")
    column = lax.axis_index("tp")
    last = sections - 1
    pair, length = inbox.shape[1:3]
    width, lru_width = w_in.shape
    parts = recv_sem.shape[1]
    core = lax.rem(column, pair)
    lead = pair - 1
    leads = core == lead
    first_stop = leads & (section == 0)
    last_stop = leads & (section == last)

    def at(stop, core_index):
        return {"pp": stop, "tp": column - core + core_index}

    def across(part):
        return slice(part * width // parts, (part + 1) * width // parts)

    barrier = pltpu.get_barrier_semaphore()

    def tell(stop, core_index):
        pl.semaphore_signal(
            barrier, inc=1, device_id=at(stop, core_index), device_id_type=MESH
        )

    def load(src, dst, index):
        return pltpu.make_async_copy(src, dst, load_sem.at[index])

    own = load(tokens_hbm.at[0, 0], mine, 0)
    small = [
        load(grate_hbm.at[0], grate, 1),
        load(ginput_hbm.at[0], ginput, 2),
        load(taps_hbm.at[0], taps, 3),
        load(cbias_hbm, cbias, 4),
        load(brate_hbm, brate, 5),
        load(binput_hbm, binput, 6),
        load(dparam_hbm, dparam, 7),
        load(gain_hbm, gain, 8),
        load(shift_hbm, shift, 9),
    ]
    load_out = load(w_out_hbm.at[0], w_out, 10)
    load_in = [
        load(w_in_hbm.at[0, across(part)], w_in.at[across(part)], 11 + part)
        for part in range(parts)
    ]
    own.start()

    @pl.when(first_stop)
    def _():
        for stop in reversed(range(sections)):
            for core_index in range(pair):
                if (stop, core_index) != (0, lead):
                    tell(stop, core_index)

    @pl.when(jnp.logical_not(first_stop | last_stop))
    def _():
        tell(last, lead)

    @pl.when(leads & (section > 0) & (section + 1 < last))
    def _():
        tell(section + 1, lead)

    heard = jnp.where(
        last_stop, sections * pair - 1, jnp.where(leads & (section > 1), 2, 1)
    ).astype(jnp.int32)

    @pl.when(leads)
    def _():
        for copy in small:
            copy.start()
        for copy in load_in:
            copy.start()
        load_out.start()

    own.wait()

    def entry(part):
        return pltpu.make_async_remote_copy(
            src_ref=mine.at[:, across(part)],
            dst_ref=inbox.at[section, core, :, across(part)],
            send_sem=entry_sem,
            recv_sem=recv_sem.at[section, part],
            device_id=at(0, lead),
            device_id_type=MESH,
        )

    @pl.when(jnp.logical_not(first_stop))
    def _():
        pl.semaphore_wait(barrier, heard)
        for part in range(parts):
            entry(part).start()

    @pl.when(leads & (section > 0))
    def _():
        pl.semaphore_signal(
            ready_sem, inc=1, device_id=at(section - 1, lead), device_id_type=MESH
        )

    def arrival(slot, part, cores):
        return pltpu.make_async_remote_copy(
            src_ref=outbox.at[slot, cores, :, across(part)],
            dst_ref=inbox.at[slot, cores, :, across(part)],
            send_sem=entry_sem,
            recv_sem=recv_sem.at[slot, part],
            device_id=at(0, lead),
            device_id_type=MESH,
        )

    def onward(slot, part):
        return pltpu.make_async_remote_copy(
            src_ref=outbox.at[slot, :, :, across(part)],
            dst_ref=inbox.at[slot, :, :, across(part)],
            send_sem=send_sem.at[slot],
            recv_sem=recv_sem.at[slot, part],
            device_id=at(jnp.minimum(section + 1, last), lead),
            device_id_type=MESH,
        )

    def onward_all(slot):
        return pltpu.make_async_remote_copy(
            src_ref=outbox.at[slot],
            dst_ref=inbox.at[slot],
            send_sem=send_sem.at[slot],
            recv_sem=recv_sem.at[slot, 0],
            device_id=at(jnp.minimum(section + 1, last), lead),
            device_id_type=MESH,
        )

    def home(slot, core_index):
        return pltpu.make_async_remote_copy(
            src_ref=outbox.at[slot, core_index],
            dst_ref=out_ref.at[0, 0],
            send_sem=send_sem.at[slot],
            recv_sem=final_sem,
            device_id=at(slot, core_index),
            device_id_type=MESH,
        )

    def homes_sent(slot, cores):
        return pltpu.make_async_remote_copy(
            src_ref=outbox.at[slot, cores],
            dst_ref=inbox.at[slot, cores],
            send_sem=send_sem.at[slot],
            recv_sem=final_sem,
            device_id=at(slot, lead),
            device_id_type=MESH,
        )

    def run_section():
        blocks, block_width, _ = grate.shape
        group = max(1, min(blocks, mxu_width // block_width))
        wide = group * block_width
        rate_map[...] = jnp.zeros_like(rate_map)
        input_map[...] = jnp.zeros_like(input_map)
        for copy in small:
            copy.wait()
        for block in range(blocks):
            to = (block % group) * block_width
            rate_map[block // group, to : to + block_width, to : to + block_width] = grate[block]
            input_map[block // group, to : to + block_width, to : to + block_width] = ginput[block]
        minus_decay = -dparam[...]
        softplus = jnp.maximum(minus_decay, 0.0) + jnp.log1p(jnp.exp(-jnp.abs(minus_decay)))
        dparam[...] = -decay_scale * softplus

        @pl.when(section == 0)
        def _():
            inbox[0, lead] = mine[...]

        position = lax.broadcasted_iota(jnp.int32, (pair, length, lru_width), 1)

        def delayed(x, by, fill):
            return jnp.where(position >= by, pltpu.roll(x, by, 1), fill)

        def one_slot(slot, carry):
            rows = pair * length
            projected = jnp.zeros((rows, lru_width), jnp.float32)
            streams = []
            entering = (section == 0) & (slot == 0)
            for part in range(parts):
                @pl.when(slot == 0)
                def _():
                    load_in[part].wait()

                @pl.when(jnp.logical_not(entering))
                def _():
                    arrival(slot, part, slice(0, pair)).wait_recv()

                if lead:
                    @pl.when(entering)
                    def _():
                        arrival(slot, part, slice(0, lead)).wait_recv()

                piece = inbox[slot, :, :, across(part)].astype(jnp.float32).reshape(rows, -1)
                streams.append(piece)
                projected = projected + jnp.dot(
                    piece.astype(jnp.bfloat16),
                    w_in[across(part), :],
                    preferred_element_type=jnp.float32,
                )
            stream = jnp.concatenate(streams, axis=1)
            projected = projected.astype(jnp.bfloat16).astype(jnp.float32)
            projected = projected.reshape(pair, length, lru_width)
            tap_count = taps.shape[0]
            convolved = cbias[...][None]
            for tap in range(tap_count):
                by = tap_count - 1 - tap
                shifted = delayed(projected, by, 0.0) if by else projected
                convolved = convolved + shifted * taps[tap : tap + 1][None]
            convolved = convolved.reshape(rows, lru_width).astype(jnp.bfloat16)

            def mapped(maps):
                return jnp.concatenate(
                    [
                        jnp.dot(
                            convolved[:, i * wide : (i + 1) * wide],
                            maps[i],
                            preferred_element_type=jnp.float32,
                        )
                        for i in range(blocks // group)
                    ],
                    axis=1,
                )

            rate_gate = jax.nn.sigmoid(mapped(rate_map) + brate[...])
            input_gate = jax.nn.sigmoid(mapped(input_map) + binput[...])
            log_decay = rate_gate * dparam[...]
            decay = jnp.exp(log_decay)
            scale_in = jnp.sqrt(-jnp.tanh(log_decay) * (decay * decay + 1.0))
            hidden = scale_in * input_gate * convolved.astype(jnp.float32)
            hidden = hidden.reshape(pair, length, lru_width)
            decay = decay.reshape(pair, length, lru_width)
            by = 1
            while by < length:
                hidden = decay * delayed(hidden, by, 0.0) + hidden
                if 2 * by < length:
                    decay = decay * delayed(decay, by, 1.0)
                by *= 2
            @pl.when(slot == 0)
            def _():
                load_out.wait()

            mixed = hidden.reshape(rows, lru_width).astype(jnp.bfloat16)
            summed = stream + jnp.dot(mixed, w_out[...], preferred_element_type=jnp.float32)
            away = summed - jnp.mean(stream, axis=-1, keepdims=True)
            offset = jnp.mean(away, axis=-1, keepdims=True)
            square = jnp.mean(away * away, axis=-1, keepdims=True)
            variance = jnp.maximum(square - offset * offset, 0.0)
            normed = (away - offset) * lax.rsqrt(variance + norm_eps) * gain[...] + shift[...]
            outbox[slot] = normed.reshape(pair, length, -1).astype(jnp.bfloat16)

            @pl.when((section < last) & (slot == 0))
            def _():
                pl.semaphore_wait(ready_sem, 1)

            @pl.when(section < last)
            def _():
                for part in range(parts):
                    onward(slot, part).start()

            @pl.when(section == last)
            def _():
                for core_index in range(pair):
                    if core_index == lead:
                        @pl.when(slot < last)
                        def _():
                            home(slot, core_index).start()

                        @pl.when(slot == last)
                        def _():
                            out_ref[0, 0] = outbox[slot, core_index]
                    else:
                        home(slot, core_index).start()

            return carry

        lax.fori_loop(0, sections, one_slot, 0)

        @pl.when(section < last)
        def _():
            for slot in range(sections):
                onward_all(slot).wait_send()

        @pl.when(section == last)
        def _():
            for slot in range(last):
                homes_sent(slot, slice(0, pair)).wait_send()
            if lead:
                homes_sent(last, slice(0, lead)).wait_send()

    pl.when(leads)(run_section)

    @pl.when(jnp.logical_not(first_stop))
    def _():
        pltpu.make_async_remote_copy(
            src_ref=mine,
            dst_ref=inbox.at[section, core],
            send_sem=entry_sem,
            recv_sem=recv_sem.at[section, 0],
            device_id=at(0, lead),
            device_id_type=MESH,
        ).wait_send()

    @pl.when(jnp.logical_not(last_stop))
    def _():
        home(0, 0).wait_recv()


def shards(sections, pair, tokens_in, *weights):
    _, _, length, width = tokens_in.shape
    lru_width = weights[0].shape[2]
    tap_count = weights[1].shape[1]
    _, blocks, block_width, _ = weights[3].shape
    group = max(1, min(blocks, mxu_width // block_width))
    wide = group * block_width
    vmem = pltpu.VMEM
    f32, bf16 = jnp.float32, jnp.bfloat16
    return pl.pallas_call(
        functools.partial(stack_kernel, sections),
        out_shape=pltpu.VMEM(tokens_in.shape, tokens_in.dtype),
        in_specs=[pl.BlockSpec(memory_space=pl.ANY)] * (1 + len(weights)),
        out_specs=pl.BlockSpec(memory_space=pltpu.VMEM),
        scratch_shapes=[
            vmem((width, lru_width), bf16),
            vmem((lru_width, width), bf16),
            vmem((tap_count, lru_width), f32),
            vmem((1, lru_width), f32),
            vmem((blocks, block_width, block_width), bf16),
            vmem((1, lru_width), f32),
            vmem((blocks, block_width, block_width), bf16),
            vmem((1, lru_width), f32),
            vmem((1, lru_width), f32),
            vmem((1, width), f32),
            vmem((1, width), f32),
            vmem((blocks // group, wide, wide), bf16),
            vmem((blocks // group, wide, wide), bf16),
            vmem((length, width), bf16),
            vmem((sections, pair, length, width), bf16),
            vmem((sections, pair, length, width), bf16),
            pltpu.SemaphoreType.DMA((11 + stream_parts,)),
            pltpu.SemaphoreType.DMA,
            pltpu.SemaphoreType.DMA((sections,)),
            pltpu.SemaphoreType.DMA((sections, stream_parts)),
            pltpu.SemaphoreType.DMA,
            pltpu.SemaphoreType.REGULAR,
        ],
        compiler_params=pltpu.CompilerParams(collective_id=0, has_side_effects=True),
        name="section_stack",
    )(tokens_in, *weights)


def solution(mesh):
    placed = (
        P("pp", ("fs", "tp"), None, None),
        P("pp", None, None),
        P("pp", None, None),
        P("pp", None),
        P("pp", None, None, None),
        P("pp", None),
        P("pp", None, None, None),
        P("pp", None),
        P("pp", None),
        P("pp", None, None),
        P("pp", None),
        P("pp", None),
    )
    pair = 2 if mesh.shape["tp"] % 2 == 0 else 1
    return jax.shard_map(
        functools.partial(shards, mesh.shape["pp"], pair),
        mesh=mesh,
        in_specs=placed,
        out_specs=P("pp", ("fs", "tp"), None, None),
        check_vma=False,
    )
```

```python
import functools

import jax
import jax.numpy as jnp
from jax import lax
from jax.experimental import pallas as pl
from jax.experimental.pallas import tpu as pltpu
from jax.sharding import PartitionSpec as P

decay_scale = 8.0
norm_eps = 1e-05
mxu_width = 256
mxus = 2
lanes = 128
MESH = pl.DeviceIdType.MESH


def fold_lanes(x):
    total = x[:, :lanes]
    for start in range(lanes, x.shape[1], lanes):
        total = total + x[:, start : start + lanes]
    return total


def stack_kernel(
    sections,
    tokens_hbm,
    w_in_hbm,
    taps_hbm,
    cbias_hbm,
    grate_hbm,
    brate_hbm,
    ginput_hbm,
    binput_hbm,
    dparam_hbm,
    w_out_hbm,
    gain_hbm,
    shift_hbm,
    out_ref,
    w_in,
    w_out,
    taps,
    channel,
    gates,
    norm,
    before,
    maps,
    folded,
    base,
    mine,
    inbox,
    outbox,
    load_sem,
    entry_sem,
    send_sem,
    recv_sem,
    final_sem,
    norm_sem,
    ready_sem,
):
    section = lax.axis_index("pp")
    column = lax.axis_index("tp")
    last = sections - 1
    pair, length = inbox.shape[1:3]
    rows = pair * length
    width, lru_width = w_in.shape
    parts = recv_sem.shape[1]
    part_width = width // parts
    tiles_in = width // mxu_width
    core = lax.rem(column, pair)
    lead = pair - 1
    leads = core == lead
    first_stop = leads & (section == 0)
    last_stop = leads & (section == last)

    def at(stop, core_index):
        return {"pp": stop, "tp": column - core + core_index}

    def across(part):
        return slice(part * part_width, (part + 1) * part_width)

    barrier = pltpu.get_barrier_semaphore()

    def tell(stop, core_index):
        pl.semaphore_signal(
            barrier, inc=1, device_id=at(stop, core_index), device_id_type=MESH
        )

    def load(src, dst, index):
        return pltpu.make_async_copy(src, dst, load_sem.at[index])

    own = load(tokens_hbm.at[0, 0], mine, 0)
    small = [
        load(grate_hbm.at[0], gates.at[0], 1),
        load(ginput_hbm.at[0], gates.at[1], 2),
        load(taps_hbm.at[0], taps, 3),
        load(cbias_hbm, channel.at[0], 4),
        load(brate_hbm, channel.at[1], 5),
        load(binput_hbm, channel.at[2], 6),
        load(dparam_hbm, channel.at[3], 7),
        load(gain_hbm, norm.at[0], 8),
        load(shift_hbm, norm.at[1], 9),
    ]
    load_in = load(w_in_hbm.at[0], w_in, 10)
    load_out = load(w_out_hbm.at[0], w_out, 11)
    own.start()

    @pl.when(first_stop)
    def _():
        for stop in reversed(range(sections)):
            for core_index in range(pair):
                if (stop, core_index) != (0, lead):
                    tell(stop, core_index)

    @pl.when(jnp.logical_not(first_stop | last_stop))
    def _():
        tell(last, lead)

    @pl.when(leads & (section > 0) & (section + 1 < last))
    def _():
        tell(section + 1, lead)

    heard = jnp.where(
        last_stop, sections * pair - 1, jnp.where(leads & (section > 1), 2, 1)
    ).astype(jnp.int32)

    @pl.when(leads)
    def _():
        for copy in small:
            copy.start()
        load_in.start()
        load_out.start()

    @pl.when(jnp.logical_not(first_stop))
    def _():
        pl.semaphore_wait(barrier, heard)

    @pl.when(leads & (section > 0))
    def _():
        pl.semaphore_signal(
            ready_sem, inc=1, device_id=at(section - 1, lead), device_id_type=MESH
        )

    own.wait()

    def entry(part):
        return pltpu.make_async_remote_copy(
            src_ref=mine.at[:, across(part)],
            dst_ref=inbox.at[section, core, :, across(part)],
            send_sem=entry_sem,
            recv_sem=recv_sem.at[section, part],
            device_id=at(0, lead),
            device_id_type=MESH,
        )

    @pl.when(jnp.logical_not(first_stop))
    def _():
        for part in range(parts):
            entry(part).start()

    def arrival(slot, part, cores):
        return pltpu.make_async_remote_copy(
            src_ref=outbox.at[slot, cores, :, across(part)],
            dst_ref=inbox.at[slot, cores, :, across(part)],
            send_sem=entry_sem,
            recv_sem=recv_sem.at[slot, part],
            device_id=at(0, lead),
            device_id_type=MESH,
        )

    def onward(slot, part):
        return pltpu.make_async_remote_copy(
            src_ref=outbox.at[slot, :, :, across(part)],
            dst_ref=inbox.at[slot, :, :, across(part)],
            send_sem=send_sem.at[slot],
            recv_sem=recv_sem.at[slot, part],
            device_id=at(jnp.minimum(section + 1, last), lead),
            device_id_type=MESH,
        )

    def onward_all(slot):
        return pltpu.make_async_remote_copy(
            src_ref=outbox.at[slot],
            dst_ref=inbox.at[slot],
            send_sem=send_sem.at[slot],
            recv_sem=recv_sem.at[slot, 0],
            device_id=at(jnp.minimum(section + 1, last), lead),
            device_id_type=MESH,
        )

    def home(slot, core_index):
        return pltpu.make_async_remote_copy(
            src_ref=outbox.at[slot, core_index],
            dst_ref=out_ref.at[0, 0],
            send_sem=send_sem.at[slot],
            recv_sem=final_sem,
            device_id=at(slot, core_index),
            device_id_type=MESH,
        )

    def homes_sent(slot, cores):
        return pltpu.make_async_remote_copy(
            src_ref=outbox.at[slot, cores],
            dst_ref=inbox.at[slot, cores],
            send_sem=send_sem.at[slot],
            recv_sem=final_sem,
            device_id=at(slot, lead),
            device_id_type=MESH,
        )

    norm_onward = pltpu.make_async_remote_copy(
        src_ref=norm,
        dst_ref=before,
        send_sem=norm_sem.at[0],
        recv_sem=norm_sem.at[1],
        device_id=at(jnp.minimum(section + 1, last), lead),
        device_id_type=MESH,
    )

    def tile(ref, row, col):
        return ref[
            row * mxu_width : (row + 1) * mxu_width,
            col * mxu_width : (col + 1) * mxu_width,
        ]

    def unit(index, mxu):
        index = index % (tiles_in + 2 + mxus * parts)
        if index < tiles_in:
            return tile(w_in, index, mxu)
        index -= tiles_in
        if index < 2:
            return maps[index, mxu]
        index -= 2
        return tile(w_out, index % mxus, (index // mxus) * mxus + mxu)

    def stage(index, mxu):
        pltpu.matmul_push_rhs(unit(index, mxu), staging_register=index % 2, mxu_index=mxu)

    def step(index, accs, lhs):
        for mxu in range(mxus):
            pltpu.matmul_acc_lhs(accs[mxu], lhs[mxu], load_staged_rhs=index % 2)
        for mxu in range(mxus):
            stage(index + 2, mxu)

    def popped(accs):
        return jnp.concatenate([pltpu.matmul_pop(acc) for acc in accs], axis=1)

    def run_section(acc_in, acc_rate, acc_input, acc_out):
        def drain():
            nothing = jnp.zeros((rows, mxu_width), jnp.bfloat16)
            for mxu in range(mxus):
                for register in range(2):
                    pltpu.matmul_acc_lhs(acc_in[mxu], nothing, load_staged_rhs=register)
            popped(acc_in)

        drain()
        for accs in (acc_rate, acc_input, *acc_out):
            popped(accs)
        _, blocks, block_width, _ = gates.shape
        group = mxu_width // block_width
        maps[...] = jnp.zeros_like(maps)
        for copy in small:
            copy.wait()

        @pl.when(section < last)
        def _():
            pl.semaphore_wait(ready_sem, 1)
            norm_onward.start()

        for gate in range(2):
            for block in range(blocks):
                to = (block % group) * block_width
                maps[gate, block // group, to : to + block_width, to : to + block_width] = gates[
                    gate, block
                ]
        minus_decay = -channel[3]
        softplus = jnp.maximum(minus_decay, 0.0) + jnp.log1p(jnp.exp(-jnp.abs(minus_decay)))
        channel[3] = -decay_scale * softplus
        load_in.wait()

        @pl.when(section == 0)
        def _():
            inbox[0, lead] = mine[...]
            before[0] = jnp.ones_like(before[0])
            before[1] = jnp.zeros_like(before[1])
            folded[...] = jnp.zeros_like(folded)

        @pl.when(section > 0)
        def _():
            norm_onward.wait_recv()
            which = lax.broadcasted_iota(jnp.int32, (rows, mxu_width), 0)
            for k in range(tiles_in):
                cols = slice(k * mxu_width, (k + 1) * mxu_width)
                split = []
                for vector in range(2):
                    value = before[vector, :, cols]
                    high = value.astype(jnp.bfloat16).astype(jnp.float32)
                    split += [high, value - high]
                lhs = jnp.zeros((rows, mxu_width), jnp.float32)
                for row, value in enumerate(split):
                    lhs = jnp.where(which == row, value, lhs)
                lhs = lhs.astype(jnp.bfloat16)
                for mxu in range(mxus):
                    stage(k, mxu)
                    pltpu.matmul_acc_lhs(acc_in[mxu], lhs, load_staged_rhs=k % 2)
            result = popped(acc_in)
            folded[0] = result[0:1] + result[1:2]
            folded[1] = result[2:3] + result[3:4]
            before[1] = before[1] - jnp.mean(before[1])

        load_out.wait()
        for mxu in range(mxus):
            stage(0, mxu)
            stage(1, mxu)
        position = lax.broadcasted_iota(jnp.int32, (pair, length, lru_width), 1)

        def delayed(x, by, fill):
            return jnp.where(position >= by, pltpu.roll(x, by, 1), fill)

        def one_slot(slot, carry):
            entering = (section == 0) & (slot == 0)
            total = jnp.zeros((rows, lanes), jnp.float32)
            squares = jnp.zeros((rows, lanes), jnp.float32)
            index = 0
            for part in range(parts):
                @pl.when(jnp.logical_not(entering))
                def _():
                    arrival(slot, part, slice(0, pair)).wait_recv()

                if lead:
                    @pl.when(entering)
                    def _():
                        arrival(slot, part, slice(0, lead)).wait_recv()

                raw = inbox[slot, :, :, across(part)].astype(jnp.float32).reshape(rows, -1)
                total = total + fold_lanes(raw)
                squares = squares + fold_lanes(raw * raw)
                scaled = (raw * before[0, :, across(part)]).astype(jnp.bfloat16)
                for start in range(0, part_width, mxu_width):
                    lhs = scaled[:, start : start + mxu_width]
                    step(index, acc_in, [lhs] * mxus)
                    index += 1
            mean = jnp.sum(total, axis=-1, keepdims=True) / width
            square = jnp.sum(squares, axis=-1, keepdims=True) / width
            variance = jnp.maximum(square - mean * mean, 0.0)
            scale = jnp.where(section > 0, lax.rsqrt(variance + norm_eps), 1.0)
            lower = scale * mean
            projected = popped(acc_in) * scale - lower * folded[0] + folded[1]
            projected = projected.astype(jnp.bfloat16).astype(jnp.float32)
            projected = projected.reshape(pair, length, lru_width)
            tap_count = taps.shape[0]
            convolved = channel[0][None]
            for tap in range(tap_count):
                by = tap_count - 1 - tap
                shifted = delayed(projected, by, 0.0) if by else projected
                convolved = convolved + shifted * taps[tap : tap + 1][None]
            convolved = convolved.reshape(rows, lru_width).astype(jnp.bfloat16)
            lhs = [convolved[:, m * mxu_width : (m + 1) * mxu_width] for m in range(mxus)]
            step(index, acc_rate, lhs)
            step(index + 1, acc_input, lhs)
            index += 2
            for part in range(parts):
                raw = inbox[slot, :, :, across(part)].astype(jnp.float32).reshape(rows, -1)
                gain, shift = before[0, :, across(part)], before[1, :, across(part)]
                base[:, across(part)] = (raw * scale - lower) * gain + shift
            rate_gate = jax.nn.sigmoid(popped(acc_rate) + channel[1])
            input_gate = jax.nn.sigmoid(popped(acc_input) + channel[2])
            log_decay = rate_gate * channel[3]
            decay = jnp.exp(log_decay)
            scale_in = jnp.sqrt(-jnp.tanh(log_decay) * (decay * decay + 1.0))
            hidden = scale_in * input_gate * convolved.astype(jnp.float32)
            hidden = hidden.reshape(pair, length, lru_width)
            decay = decay.reshape(pair, length, lru_width)
            by = 1
            while by < length:
                hidden = decay * delayed(hidden, by, 0.0) + hidden
                if 2 * by < length:
                    decay = decay * delayed(decay, by, 1.0)
                by *= 2
            mixed = hidden.reshape(rows, lru_width).astype(jnp.bfloat16)

            def project(part):
                for k in range(mxus):
                    lhs = mixed[:, k * mxu_width : (k + 1) * mxu_width]
                    step(index + mxus * part + k, acc_out[part], [lhs] * mxus)

            def finish(part):
                away = base[:, across(part)] + popped(acc_out[part])
                base[:, across(part)] = away
                outbox[slot, :, :, across(part)] = away.reshape(pair, length, -1).astype(
                    jnp.bfloat16
                )

                @pl.when(section < last)
                def _():
                    onward(slot, part).start()

            project(0)
            for part in range(1, parts):
                project(part)
                finish(part - 1)
            finish(parts - 1)

            @pl.when(section == last)
            def _():
                away = base[...]
                offset = jnp.sum(fold_lanes(away), axis=-1, keepdims=True) / width
                square = jnp.sum(fold_lanes(away * away), axis=-1, keepdims=True) / width
                variance = jnp.maximum(square - offset * offset, 0.0)
                normed = (away - offset) * lax.rsqrt(variance + norm_eps) * norm[0] + norm[1]
                outbox[slot] = normed.reshape(pair, length, -1).astype(jnp.bfloat16)
                for core_index in range(pair):
                    if core_index == lead:
                        @pl.when(slot < last)
                        def _():
                            home(slot, core_index).start()

                        @pl.when(slot == last)
                        def _():
                            out_ref[0, 0] = outbox[slot, core_index]
                    else:
                        home(slot, core_index).start()

            return carry

        lax.fori_loop(0, sections, one_slot, 0)
        drain()

        @pl.when(section < last)
        def _():
            norm_onward.wait_send()
            for slot in range(sections):
                onward_all(slot).wait_send()

        @pl.when(section == last)
        def _():
            for slot in range(last):
                homes_sent(slot, slice(0, pair)).wait_send()
            if lead:
                homes_sent(last, slice(0, lead)).wait_send()

    def with_accumulators(*accs):
        pairs = [accs[start : start + mxus] for start in range(0, len(accs), mxus)]

        @pl.when(leads)
        def _():
            run_section(pairs[0], pairs[1], pairs[2], pairs[3:])

    pl.run_scoped(
        with_accumulators,
        *[
            pltpu.ACC(mxu)((rows, mxu_width), jnp.float32)
            for _ in range(3 + parts)
            for mxu in range(mxus)
        ],
    )

    @pl.when(jnp.logical_not(first_stop))
    def _():
        pltpu.make_async_remote_copy(
            src_ref=mine,
            dst_ref=inbox.at[section, core],
            send_sem=entry_sem,
            recv_sem=recv_sem.at[section, 0],
            device_id=at(0, lead),
            device_id_type=MESH,
        ).wait_send()

    @pl.when(jnp.logical_not(last_stop))
    def _():
        home(0, 0).wait_recv()


def shards(sections, pair, tokens_in, *weights):
    _, _, length, width = tokens_in.shape
    lru_width = weights[0].shape[2]
    tap_count = weights[1].shape[1]
    _, blocks, block_width, _ = weights[3].shape
    parts = width // (mxus * mxu_width)
    assert lru_width == mxus * mxu_width and mxu_width % block_width == 0
    vmem = pltpu.VMEM
    f32, bf16 = jnp.float32, jnp.bfloat16
    return pl.pallas_call(
        functools.partial(stack_kernel, sections),
        out_shape=pltpu.VMEM(tokens_in.shape, tokens_in.dtype),
        in_specs=[pl.BlockSpec(memory_space=pl.ANY)] * (1 + len(weights)),
        out_specs=pl.BlockSpec(memory_space=pltpu.VMEM),
        scratch_shapes=[
            vmem((width, lru_width), bf16),
            vmem((lru_width, width), bf16),
            vmem((tap_count, lru_width), f32),
            vmem((4, 1, lru_width), f32),
            vmem((2, blocks, block_width, block_width), bf16),
            vmem((2, 1, width), f32),
            vmem((2, 1, width), f32),
            vmem((2, mxus, mxu_width, mxu_width), bf16),
            vmem((2, 1, lru_width), f32),
            vmem((pair * length, width), f32),
            vmem((length, width), bf16),
            vmem((sections, pair, length, width), bf16),
            vmem((sections, pair, length, width), bf16),
            pltpu.SemaphoreType.DMA((12,)),
            pltpu.SemaphoreType.DMA,
            pltpu.SemaphoreType.DMA((sections,)),
            pltpu.SemaphoreType.DMA((sections, parts)),
            pltpu.SemaphoreType.DMA,
            pltpu.SemaphoreType.DMA((2,)),
            pltpu.SemaphoreType.REGULAR,
        ],
        compiler_params=pltpu.CompilerParams(collective_id=0, has_side_effects=True),
        name="section_stack",
    )(tokens_in, *weights)


def solution(mesh):
    placed = (
        P("pp", ("fs", "tp"), None, None),
        P("pp", None, None),
        P("pp", None, None),
        P("pp", None),
        P("pp", None, None, None),
        P("pp", None),
        P("pp", None, None, None),
        P("pp", None),
        P("pp", None),
        P("pp", None, None),
        P("pp", None),
        P("pp", None),
    )
    pair = 2 if mesh.shape["tp"] % 2 == 0 else 1
    return jax.shard_map(
        functools.partial(shards, mesh.shape["pp"], pair),
        mesh=mesh,
        in_specs=placed,
        out_specs=P("pp", ("fs", "tp"), None, None),
        check_vma=False,
    )
```

```python
import functools

import jax
import jax.numpy as jnp
from jax import lax
from jax.experimental import pallas as pl
from jax.experimental.pallas import tpu as pltpu
from jax.sharding import PartitionSpec as P

decay_scale = 8.0
norm_eps = 1e-05
mxu_width = 256
mxus = 2
lanes = 128
MESH = pl.DeviceIdType.MESH


def fold_lanes(x):
    total = x[:, :lanes]
    for start in range(lanes, x.shape[1], lanes):
        total = total + x[:, start : start + lanes]
    return total


def stack_kernel(
    sections,
    tokens_hbm,
    w_in_hbm,
    taps_hbm,
    cbias_hbm,
    grate_hbm,
    brate_hbm,
    ginput_hbm,
    binput_hbm,
    dparam_hbm,
    w_out_hbm,
    gain_hbm,
    shift_hbm,
    out_ref,
    w_in,
    w_out,
    taps,
    channel,
    gates,
    norm,
    before,
    maps,
    folded,
    base,
    inbox,
    outbox,
    load_sem,
    entry_sem,
    send_sem,
    recv_sem,
    final_sem,
    norm_sem,
    ready_sem,
):
    section = lax.axis_index("pp")
    column = lax.axis_index("tp")
    last = sections - 1
    pair, length = inbox.shape[1:3]
    rows = pair * length
    width, lru_width = w_in.shape
    parts = recv_sem.shape[1]
    part_width = width // parts
    tiles_in = width // mxu_width
    core = lax.rem(column, pair)
    lead = pair - 1
    leads = core == lead
    first_stop = leads & (section == 0)
    last_stop = leads & (section == last)

    def at(stop, core_index):
        return {"pp": stop, "tp": column - core + core_index}

    def across(part):
        return slice(part * part_width, (part + 1) * part_width)

    barrier = pltpu.get_barrier_semaphore()

    def tell(stop, core_index):
        pl.semaphore_signal(
            barrier, inc=1, device_id=at(stop, core_index), device_id_type=MESH
        )

    def load(src, dst, index):
        return pltpu.make_async_copy(src, dst, load_sem.at[index])

    own = load(tokens_hbm.at[0, 0], inbox.at[0, lead], 0)
    small = [
        load(grate_hbm.at[0], gates.at[0], 1),
        load(ginput_hbm.at[0], gates.at[1], 2),
        load(taps_hbm.at[0], taps, 3),
        load(cbias_hbm, channel.at[0], 4),
        load(brate_hbm, channel.at[1], 5),
        load(binput_hbm, channel.at[2], 6),
        load(dparam_hbm, channel.at[3], 7),
        load(gain_hbm, norm.at[0], 8),
        load(shift_hbm, norm.at[1], 9),
    ]
    load_in = [
        load(w_in_hbm.at[0, across(part)], w_in.at[across(part)], 10 + part)
        for part in range(parts)
    ]
    load_out = [
        load(w_out_hbm.at[0, :, across(part)], w_out.at[:, across(part)], 10 + parts + part)
        for part in range(parts)
    ]

    @pl.when(first_stop)
    def _():
        for stop in reversed(range(sections)):
            for core_index in range(pair):
                if (stop, core_index) != (0, lead):
                    tell(stop, core_index)

    @pl.when(jnp.logical_not(first_stop | last_stop))
    def _():
        tell(last, lead)

    @pl.when(leads & (section > 0) & (section + 1 < last))
    def _():
        tell(section + 1, lead)

    heard = jnp.where(
        last_stop, sections * pair - 1, jnp.where(leads & (section > 1), 2, 1)
    ).astype(jnp.int32)

    def entry(part):
        return pltpu.make_async_remote_copy(
            src_ref=tokens_hbm.at[0, 0, :, across(part)],
            dst_ref=inbox.at[section, core, :, across(part)],
            send_sem=entry_sem,
            recv_sem=recv_sem.at[section, part],
            device_id=at(0, lead),
            device_id_type=MESH,
        )

    @pl.when(jnp.logical_not(first_stop))
    def _():
        pl.semaphore_wait(barrier, heard)
        for part in range(parts):
            entry(part).start()

    @pl.when(first_stop)
    def _():
        own.start()

    @pl.when(leads & (section > 0))
    def _():
        pl.semaphore_signal(
            ready_sem, inc=1, device_id=at(section - 1, lead), device_id_type=MESH
        )

    @pl.when(leads)
    def _():
        for copy in small[:3]:
            copy.start()
        for copy in load_in:
            copy.start()
        for copy in small[3:] + load_out:
            copy.start()

    def arrival(slot, part, cores):
        return pltpu.make_async_remote_copy(
            src_ref=outbox.at[slot, cores, :, across(part)],
            dst_ref=inbox.at[slot, cores, :, across(part)],
            send_sem=entry_sem,
            recv_sem=recv_sem.at[slot, part],
            device_id=at(0, lead),
            device_id_type=MESH,
        )

    def onward(slot, part):
        return pltpu.make_async_remote_copy(
            src_ref=outbox.at[slot, :, :, across(part)],
            dst_ref=inbox.at[slot, :, :, across(part)],
            send_sem=send_sem.at[slot],
            recv_sem=recv_sem.at[slot, part],
            device_id=at(jnp.minimum(section + 1, last), lead),
            device_id_type=MESH,
        )

    def onward_all(slot):
        return pltpu.make_async_remote_copy(
            src_ref=outbox.at[slot],
            dst_ref=inbox.at[slot],
            send_sem=send_sem.at[slot],
            recv_sem=recv_sem.at[slot, 0],
            device_id=at(jnp.minimum(section + 1, last), lead),
            device_id_type=MESH,
        )

    def home(slot, core_index):
        return pltpu.make_async_remote_copy(
            src_ref=outbox.at[slot, core_index],
            dst_ref=out_ref.at[0, 0],
            send_sem=send_sem.at[slot],
            recv_sem=final_sem,
            device_id=at(slot, core_index),
            device_id_type=MESH,
        )

    def homes_sent(slot, cores):
        return pltpu.make_async_remote_copy(
            src_ref=outbox.at[slot, cores],
            dst_ref=inbox.at[slot, cores],
            send_sem=send_sem.at[slot],
            recv_sem=final_sem,
            device_id=at(slot, lead),
            device_id_type=MESH,
        )

    norm_onward = pltpu.make_async_remote_copy(
        src_ref=norm,
        dst_ref=before,
        send_sem=norm_sem.at[0],
        recv_sem=norm_sem.at[1],
        device_id=at(jnp.minimum(section + 1, last), lead),
        device_id_type=MESH,
    )

    def tile(ref, row, col):
        return ref[
            row * mxu_width : (row + 1) * mxu_width,
            col * mxu_width : (col + 1) * mxu_width,
        ]

    def unit(index, mxu):
        index = index % (tiles_in + 2 + mxus * parts)
        if index < tiles_in:
            return tile(w_in, index, mxu)
        index -= tiles_in
        if index < 2:
            return maps[index, mxu]
        index -= 2
        return tile(w_out, index % mxus, (index // mxus) * mxus + mxu)

    def stage(index, mxu):
        pltpu.matmul_push_rhs(unit(index, mxu), staging_register=index % 2, mxu_index=mxu)

    def step(index, accs, lhs):
        for mxu in range(mxus):
            pltpu.matmul_acc_lhs(accs[mxu], lhs[mxu], load_staged_rhs=index % 2)
        for mxu in range(mxus):
            stage(index + 2, mxu)

    def popped(accs):
        return jnp.concatenate([pltpu.matmul_pop(acc) for acc in accs], axis=1)

    def run_section(acc_in, acc_rate, acc_input, acc_out):
        def drain():
            nothing = jnp.zeros((rows, mxu_width), jnp.bfloat16)
            for mxu in range(mxus):
                for register in range(2):
                    pltpu.matmul_acc_lhs(acc_in[mxu], nothing, load_staged_rhs=register)
            popped(acc_in)

        drain()
        for accs in (acc_rate, acc_input, *acc_out):
            popped(accs)
        _, blocks, block_width, _ = gates.shape
        group = mxu_width // block_width
        maps[...] = jnp.zeros_like(maps)
        for copy in small:
            copy.wait()

        def norm_send():
            pl.semaphore_wait(ready_sem, 1)
            norm_onward.start()

        pl.when((section > 0) & (section < last))(norm_send)

        for gate in range(2):
            for block in range(blocks):
                to = (block % group) * block_width
                maps[gate, block // group, to : to + block_width, to : to + block_width] = gates[
                    gate, block
                ]
        minus_decay = -channel[3]
        softplus = jnp.maximum(minus_decay, 0.0) + jnp.log1p(jnp.exp(-jnp.abs(minus_decay)))
        channel[3] = -decay_scale * softplus

        @pl.when(first_stop)
        def _():
            own.wait()
            load_in[0].wait()
            before[0] = jnp.ones_like(before[0])
            before[1] = jnp.zeros_like(before[1])
            folded[...] = jnp.zeros_like(folded)

        @pl.when(section > 0)
        def _():
            for copy in load_in + load_out:
                copy.wait()
            norm_onward.wait_recv()
            which = lax.broadcasted_iota(jnp.int32, (rows, mxu_width), 0)
            for k in range(tiles_in):
                cols = slice(k * mxu_width, (k + 1) * mxu_width)
                split = []
                for vector in range(2):
                    value = before[vector, :, cols]
                    high = value.astype(jnp.bfloat16).astype(jnp.float32)
                    split += [high, value - high]
                lhs = jnp.zeros((rows, mxu_width), jnp.float32)
                for row, value in enumerate(split):
                    lhs = jnp.where(which == row, value, lhs)
                lhs = lhs.astype(jnp.bfloat16)
                for mxu in range(mxus):
                    stage(k, mxu)
                    pltpu.matmul_acc_lhs(acc_in[mxu], lhs, load_staged_rhs=k % 2)
            result = popped(acc_in)
            folded[0] = result[0:1] + result[1:2]
            folded[1] = result[2:3] + result[3:4]
            before[1] = before[1] - jnp.mean(before[1])

        for mxu in range(mxus):
            stage(0, mxu)
            stage(1, mxu)
        position = lax.broadcasted_iota(jnp.int32, (pair, length, lru_width), 1)

        def delayed(x, by, fill):
            return jnp.where(position >= by, pltpu.roll(x, by, 1), fill)

        def one_slot(slot, carry):
            entering = (section == 0) & (slot == 0)
            total = jnp.zeros((rows, lanes), jnp.float32)
            squares = jnp.zeros((rows, lanes), jnp.float32)
            index = 0
            for part in range(parts):
                @pl.when(jnp.logical_not(entering))
                def _():
                    arrival(slot, part, slice(0, pair)).wait_recv()

                if lead:
                    @pl.when(entering)
                    def _():
                        arrival(slot, part, slice(0, lead)).wait_recv()

                raw = inbox[slot, :, :, across(part)].astype(jnp.float32).reshape(rows, -1)
                total = total + fold_lanes(raw)
                squares = squares + fold_lanes(raw * raw)
                if part + 1 < parts:
                    pl.when(entering)(load_in[part + 1].wait)
                scaled = (raw * before[0, :, across(part)]).astype(jnp.bfloat16)
                for start in range(0, part_width, mxu_width):
                    lhs = scaled[:, start : start + mxu_width]
                    step(index, acc_in, [lhs] * mxus)
                    index += 1

            mean = jnp.sum(total, axis=-1, keepdims=True) / width
            square = jnp.sum(squares, axis=-1, keepdims=True) / width
            variance = jnp.maximum(square - mean * mean, 0.0)
            scale = jnp.where(section > 0, lax.rsqrt(variance + norm_eps), 1.0)
            lower = scale * mean

            @pl.when(entering & (section < last))
            def _():
                norm_send()

            projected = popped(acc_in) * scale - lower * folded[0] + folded[1]
            projected = projected.astype(jnp.bfloat16).astype(jnp.float32)
            projected = projected.reshape(pair, length, lru_width)
            tap_count = taps.shape[0]
            convolved = channel[0][None]
            for tap in range(tap_count):
                by = tap_count - 1 - tap
                shifted = delayed(projected, by, 0.0) if by else projected
                convolved = convolved + shifted * taps[tap : tap + 1][None]
            convolved = convolved.reshape(rows, lru_width).astype(jnp.bfloat16)
            lhs = [convolved[:, m * mxu_width : (m + 1) * mxu_width] for m in range(mxus)]
            pl.when(entering)(load_out[0].wait)
            step(index, acc_rate, lhs)
            step(index + 1, acc_input, lhs)
            index += 2
            for part in range(parts):
                raw = inbox[slot, :, :, across(part)].astype(jnp.float32).reshape(rows, -1)
                gain, shift = before[0, :, across(part)], before[1, :, across(part)]
                base[:, across(part)] = (raw * scale - lower) * gain + shift
            rate_gate = jax.nn.sigmoid(popped(acc_rate) + channel[1])
            input_gate = jax.nn.sigmoid(popped(acc_input) + channel[2])
            log_decay = rate_gate * channel[3]
            decay = jnp.exp(log_decay)
            scale_in = jnp.sqrt(-jnp.tanh(log_decay) * (decay * decay + 1.0))
            hidden = scale_in * input_gate * convolved.astype(jnp.float32)
            hidden = hidden.reshape(pair, length, lru_width)
            decay = decay.reshape(pair, length, lru_width)
            by = 1
            while by < length:
                hidden = decay * delayed(hidden, by, 0.0) + hidden
                if 2 * by < length:
                    decay = decay * delayed(decay, by, 1.0)
                by *= 2
            mixed = hidden.reshape(rows, lru_width).astype(jnp.bfloat16)

            def project(part):
                if part + 1 < parts:
                    pl.when(entering)(load_out[part + 1].wait)
                for k in range(mxus):
                    lhs = mixed[:, k * mxu_width : (k + 1) * mxu_width]
                    step(index + mxus * part + k, acc_out[part], [lhs] * mxus)

            def finish(part):
                away = base[:, across(part)] + popped(acc_out[part])
                base[:, across(part)] = away
                outbox[slot, :, :, across(part)] = away.reshape(pair, length, -1).astype(
                    jnp.bfloat16
                )

                @pl.when(section < last)
                def _():
                    onward(slot, part).start()

            project(0)
            for part in range(1, parts):
                project(part)
                finish(part - 1)
            finish(parts - 1)

            @pl.when(section == last)
            def _():
                away = base[...]
                offset = jnp.sum(fold_lanes(away), axis=-1, keepdims=True) / width
                square = jnp.sum(fold_lanes(away * away), axis=-1, keepdims=True) / width
                variance = jnp.maximum(square - offset * offset, 0.0)
                normed = (away - offset) * lax.rsqrt(variance + norm_eps) * norm[0] + norm[1]
                outbox[slot] = normed.reshape(pair, length, -1).astype(jnp.bfloat16)
                for core_index in range(pair):
                    if core_index == lead:
                        @pl.when(slot < last)
                        def _():
                            home(slot, core_index).start()

                        @pl.when(slot == last)
                        def _():
                            out_ref[0, 0] = outbox[slot, core_index]
                    else:
                        home(slot, core_index).start()

            return carry

        lax.fori_loop(0, sections, one_slot, 0)
        drain()

        @pl.when(section < last)
        def _():
            norm_onward.wait_send()
            for slot in range(sections):
                onward_all(slot).wait_send()

        @pl.when(section == last)
        def _():
            for slot in range(last):
                homes_sent(slot, slice(0, pair)).wait_send()
            if lead:
                homes_sent(last, slice(0, lead)).wait_send()

    def with_accumulators(*accs):
        pairs = [accs[start : start + mxus] for start in range(0, len(accs), mxus)]

        @pl.when(leads)
        def _():
            run_section(pairs[0], pairs[1], pairs[2], pairs[3:])

    pl.run_scoped(
        with_accumulators,
        *[
            pltpu.ACC(mxu)((rows, mxu_width), jnp.float32)
            for _ in range(3 + parts)
            for mxu in range(mxus)
        ],
    )

    @pl.when(jnp.logical_not(first_stop))
    def _():
        pltpu.make_async_remote_copy(
            src_ref=tokens_hbm.at[0, 0],
            dst_ref=inbox.at[section, core],
            send_sem=entry_sem,
            recv_sem=recv_sem.at[section, 0],
            device_id=at(0, lead),
            device_id_type=MESH,
        ).wait_send()

    @pl.when(jnp.logical_not(last_stop))
    def _():
        home(0, 0).wait_recv()


def shards(sections, pair, tokens_in, *weights):
    _, _, length, width = tokens_in.shape
    lru_width = weights[0].shape[2]
    tap_count = weights[1].shape[1]
    _, blocks, block_width, _ = weights[3].shape
    parts = width // (mxus * mxu_width)
    assert lru_width == mxus * mxu_width and mxu_width % block_width == 0
    vmem = pltpu.VMEM
    f32, bf16 = jnp.float32, jnp.bfloat16
    return pl.pallas_call(
        functools.partial(stack_kernel, sections),
        out_shape=pltpu.VMEM(tokens_in.shape, tokens_in.dtype),
        in_specs=[pl.BlockSpec(memory_space=pl.ANY)] * (1 + len(weights)),
        out_specs=pl.BlockSpec(memory_space=pltpu.VMEM),
        scratch_shapes=[
            vmem((width, lru_width), bf16),
            vmem((lru_width, width), bf16),
            vmem((tap_count, lru_width), f32),
            vmem((4, 1, lru_width), f32),
            vmem((2, blocks, block_width, block_width), bf16),
            vmem((2, 1, width), f32),
            vmem((2, 1, width), f32),
            vmem((2, mxus, mxu_width, mxu_width), bf16),
            vmem((2, 1, lru_width), f32),
            vmem((pair * length, width), f32),
            vmem((sections, pair, length, width), bf16),
            vmem((sections, pair, length, width), bf16),
            pltpu.SemaphoreType.DMA((10 + 2 * parts,)),
            pltpu.SemaphoreType.DMA,
            pltpu.SemaphoreType.DMA((sections,)),
            pltpu.SemaphoreType.DMA((sections, parts)),
            pltpu.SemaphoreType.DMA,
            pltpu.SemaphoreType.DMA((2,)),
            pltpu.SemaphoreType.REGULAR,
        ],
        compiler_params=pltpu.CompilerParams(collective_id=0, has_side_effects=True),
        name="section_stack",
    )(tokens_in, *weights)


def solution(mesh):
    placed = (
        P("pp", ("fs", "tp"), None, None),
        P("pp", None, None),
        P("pp", None, None),
        P("pp", None),
        P("pp", None, None, None),
        P("pp", None),
        P("pp", None, None, None),
        P("pp", None),
        P("pp", None),
        P("pp", None, None),
        P("pp", None),
        P("pp", None),
    )
    pair = 2 if mesh.shape["tp"] % 2 == 0 else 1
    return jax.shard_map(
        functools.partial(shards, mesh.shape["pp"], pair),
        mesh=mesh,
        in_specs=placed,
        out_specs=P("pp", ("fs", "tp"), None, None),
        check_vma=False,
    )
```

```python
import functools

import jax
import jax.numpy as jnp
from jax import lax
from jax.experimental import pallas as pl
from jax.experimental.pallas import tpu as pltpu
from jax.sharding import PartitionSpec as P

decay_scale = 8.0
norm_eps = 1e-05
mxu_width = 256
mxus = 2
lanes = 128
MESH = pl.DeviceIdType.MESH


def fold_lanes(x):
    total = x[:, :lanes]
    for start in range(lanes, x.shape[1], lanes):
        total = total + x[:, start : start + lanes]
    return total


def stack_kernel(
    sections,
    tokens_hbm,
    w_in_hbm,
    taps_hbm,
    cbias_hbm,
    grate_hbm,
    brate_hbm,
    ginput_hbm,
    binput_hbm,
    dparam_hbm,
    w_out_hbm,
    gain_hbm,
    shift_hbm,
    out_ref,
    w_in,
    w_out,
    taps,
    channel,
    gates,
    norm,
    before,
    after,
    landing,
    maps,
    folded,
    base,
    inbox,
    outbox,
    load_sem,
    entry_sem,
    send_sem,
    recv_sem,
    final_sem,
    norm_sem,
    home_sem,
    ready_sem,
    *accs,
):
    section = lax.axis_index("pp")
    column = lax.axis_index("tp")
    last = sections - 1
    pair, length = inbox.shape[1:3]
    rows = pair * length
    width, lru_width = w_in.shape
    parts = recv_sem.shape[1]
    part_width = width // parts
    tiles_in = width // mxu_width
    core = lax.rem(column, pair)
    lead = pair - 1
    leads = core == lead
    first_stop = leads & (section == 0)
    last_stop = leads & (section == last)

    def at(stop, core_index):
        return {"pp": stop, "tp": column - core + core_index}

    def across(part):
        return slice(part * part_width, (part + 1) * part_width)

    barrier = pltpu.get_barrier_semaphore()

    def tell(stop, core_index):
        pl.semaphore_signal(
            barrier, inc=1, device_id=at(stop, core_index), device_id_type=MESH
        )

    def load(src, dst, index):
        return pltpu.make_async_copy(src, dst, load_sem.at[index])

    own = load(tokens_hbm.at[0, 0], inbox.at[0, lead], 0)
    small = [
        load(grate_hbm.at[0], gates.at[0], 1),
        load(ginput_hbm.at[0], gates.at[1], 2),
        load(taps_hbm.at[0], taps, 3),
        load(cbias_hbm, channel.at[0], 4),
        load(brate_hbm, channel.at[1], 5),
        load(binput_hbm, channel.at[2], 6),
        load(dparam_hbm, channel.at[3], 7),
        load(gain_hbm, norm.at[0], 8),
        load(shift_hbm, norm.at[1], 9),
    ]
    load_in = [
        load(w_in_hbm.at[0, across(part)], w_in.at[across(part)], 10 + part)
        for part in range(parts)
    ]
    load_out = [
        load(w_out_hbm.at[0, :, across(part)], w_out.at[:, across(part)], 10 + parts + part)
        for part in range(parts)
    ]

    @pl.when(first_stop)
    def _():
        for stop in reversed(range(sections)):
            for core_index in range(pair):
                if (stop, core_index) != (0, lead):
                    tell(stop, core_index)

    @pl.when(jnp.logical_not(first_stop | last_stop))
    def _():
        tell(last, lead)

    @pl.when(leads & (section > 0) & (section + 1 < last))
    def _():
        tell(section + 1, lead)

    heard = jnp.where(
        last_stop, sections * pair - 1, jnp.where(leads & (section > 1), 2, 1)
    ).astype(jnp.int32)

    def entry(part):
        return pltpu.make_async_remote_copy(
            src_ref=tokens_hbm.at[0, 0, :, across(part)],
            dst_ref=inbox.at[section, core, :, across(part)],
            send_sem=entry_sem,
            recv_sem=recv_sem.at[section, part],
            device_id=at(0, lead),
            device_id_type=MESH,
        )

    @pl.when(jnp.logical_not(first_stop))
    def _():
        pl.semaphore_wait(barrier, heard)
        for part in range(parts):
            entry(part).start()

    @pl.when(first_stop)
    def _():
        own.start()

    @pl.when(leads & (section > 0))
    def _():
        pl.semaphore_signal(
            ready_sem, inc=1, device_id=at(section - 1, lead), device_id_type=MESH
        )

    @pl.when(leads)
    def _():
        for copy in small[:3]:
            copy.start()
        for copy in load_in:
            copy.start()
        for copy in small[3:] + load_out:
            copy.start()

    def arrival(slot, part, cores):
        return pltpu.make_async_remote_copy(
            src_ref=outbox.at[slot, cores, :, across(part)],
            dst_ref=inbox.at[slot, cores, :, across(part)],
            send_sem=entry_sem,
            recv_sem=recv_sem.at[slot, part],
            device_id=at(0, lead),
            device_id_type=MESH,
        )

    def onward(slot, part):
        return pltpu.make_async_remote_copy(
            src_ref=outbox.at[slot, :, :, across(part)],
            dst_ref=inbox.at[slot, :, :, across(part)],
            send_sem=send_sem.at[slot],
            recv_sem=recv_sem.at[slot, part],
            device_id=at(jnp.minimum(section + 1, last), lead),
            device_id_type=MESH,
        )

    def onward_all(slot):
        return pltpu.make_async_remote_copy(
            src_ref=outbox.at[slot],
            dst_ref=inbox.at[slot],
            send_sem=send_sem.at[slot],
            recv_sem=recv_sem.at[slot, 0],
            device_id=at(jnp.minimum(section + 1, last), lead),
            device_id_type=MESH,
        )

    def home(slot, part, core_index):
        return pltpu.make_async_remote_copy(
            src_ref=outbox.at[slot, core_index, :, across(part)],
            dst_ref=landing.at[:, across(part)],
            send_sem=send_sem.at[slot],
            recv_sem=final_sem,
            device_id=at(slot, core_index),
            device_id_type=MESH,
        )

    def landed():
        return pltpu.make_async_remote_copy(
            src_ref=landing,
            dst_ref=landing,
            send_sem=entry_sem,
            recv_sem=final_sem,
            device_id=at(0, lead),
            device_id_type=MESH,
        )

    def norm_home(slot, core_index):
        return pltpu.make_async_remote_copy(
            src_ref=norm,
            dst_ref=after,
            send_sem=home_sem.at[slot, core_index],
            recv_sem=norm_sem.at[2],
            device_id=at(slot, core_index),
            device_id_type=MESH,
        )

    homes = [
        (slot, core_index)
        for slot in range(sections)
        for core_index in reversed(range(pair))
        if (slot, core_index) != (last, lead)
    ]

    def homes_sent(slot, cores):
        return pltpu.make_async_remote_copy(
            src_ref=outbox.at[slot, cores],
            dst_ref=inbox.at[slot, cores],
            send_sem=send_sem.at[slot],
            recv_sem=final_sem,
            device_id=at(slot, lead),
            device_id_type=MESH,
        )

    norm_onward = pltpu.make_async_remote_copy(
        src_ref=norm,
        dst_ref=before,
        send_sem=norm_sem.at[0],
        recv_sem=norm_sem.at[1],
        device_id=at(jnp.minimum(section + 1, last), lead),
        device_id_type=MESH,
    )

    def tile(ref, row, col):
        return ref[
            row * mxu_width : (row + 1) * mxu_width,
            col * mxu_width : (col + 1) * mxu_width,
        ]

    def unit(index, mxu):
        index = index % (tiles_in + 2 + mxus * parts)
        if index < tiles_in:
            return tile(w_in, index, mxu)
        index -= tiles_in
        if index < 2:
            return maps[index, mxu]
        index -= 2
        return tile(w_out, index % mxus, (index // mxus) * mxus + mxu)

    def stage(index, mxu):
        pltpu.matmul_push_rhs(unit(index, mxu), staging_register=index % 2, mxu_index=mxu)

    def step(index, accs, lhs):
        for mxu in range(mxus):
            pltpu.matmul_acc_lhs(accs[mxu], lhs[mxu], load_staged_rhs=index % 2)
        for mxu in range(mxus):
            stage(index + 2, mxu)

    def popped(accs):
        return jnp.concatenate([pltpu.matmul_pop(acc) for acc in accs], axis=1)

    def run_section(acc_in, acc_rate, acc_input, acc_out):
        def drain():
            nothing = jnp.zeros((rows, mxu_width), jnp.bfloat16)
            for mxu in range(mxus):
                for register in range(2):
                    pltpu.matmul_acc_lhs(acc_in[mxu], nothing, load_staged_rhs=register)
            popped(acc_in)

        drain()
        for accs in (acc_rate, acc_input, *acc_out):
            popped(accs)
        _, blocks, block_width, _ = gates.shape
        group = mxu_width // block_width
        maps[...] = jnp.zeros_like(maps)
        for copy in small:
            copy.wait()

        def norm_send():
            pl.semaphore_wait(ready_sem, 1)
            norm_onward.start()

        pl.when((section > 0) & (section < last))(norm_send)

        for gate in range(2):
            for block in range(blocks):
                to = (block % group) * block_width
                maps[gate, block // group, to : to + block_width, to : to + block_width] = gates[
                    gate, block
                ]
        minus_decay = -channel[3]
        softplus = jnp.maximum(minus_decay, 0.0) + jnp.log1p(jnp.exp(-jnp.abs(minus_decay)))
        channel[3] = -decay_scale * softplus

        @pl.when(first_stop)
        def _():
            own.wait()
            load_in[0].wait()
            before[0] = jnp.ones_like(before[0])
            before[1] = jnp.zeros_like(before[1])
            folded[...] = jnp.zeros_like(folded)

        @pl.when(section > 0)
        def _():
            for copy in load_in + load_out:
                copy.wait()
            norm_onward.wait_recv()
            which = lax.broadcasted_iota(jnp.int32, (rows, mxu_width), 0)
            for k in range(tiles_in):
                cols = slice(k * mxu_width, (k + 1) * mxu_width)
                split = []
                for vector in range(2):
                    value = before[vector, :, cols]
                    high = value.astype(jnp.bfloat16).astype(jnp.float32)
                    split += [high, value - high]
                lhs = jnp.zeros((rows, mxu_width), jnp.float32)
                for row, value in enumerate(split):
                    lhs = jnp.where(which == row, value, lhs)
                lhs = lhs.astype(jnp.bfloat16)
                for mxu in range(mxus):
                    stage(k, mxu)
                    pltpu.matmul_acc_lhs(acc_in[mxu], lhs, load_staged_rhs=k % 2)
            result = popped(acc_in)
            folded[0] = result[0:1] + result[1:2]
            folded[1] = result[2:3] + result[3:4]
            before[1] = before[1] - jnp.mean(before[1])

        for mxu in range(mxus):
            stage(0, mxu)
            stage(1, mxu)
        position = lax.broadcasted_iota(jnp.int32, (pair, length, lru_width), 1)

        def delayed(x, by, fill):
            return jnp.where(position >= by, pltpu.roll(x, by, 1), fill)

        @pl.when(section == last)
        def _():
            after[...] = norm[...]
            for slot, core_index in homes:
                norm_home(slot, core_index).start()

        def one_slot(slot, carry):
            entering = (section == 0) & (slot == 0)
            total = jnp.zeros((rows, lanes), jnp.float32)
            squares = jnp.zeros((rows, lanes), jnp.float32)
            index = 0
            for part in range(parts):
                @pl.when(jnp.logical_not(entering))
                def _():
                    arrival(slot, part, slice(0, pair)).wait_recv()

                if lead:
                    @pl.when(entering)
                    def _():
                        arrival(slot, part, slice(0, lead)).wait_recv()

                raw = inbox[slot, :, :, across(part)].astype(jnp.float32).reshape(rows, -1)
                total = total + fold_lanes(raw)
                squares = squares + fold_lanes(raw * raw)
                if part + 1 < parts:
                    pl.when(entering)(load_in[part + 1].wait)
                scaled = (raw * before[0, :, across(part)]).astype(jnp.bfloat16)
                for start in range(0, part_width, mxu_width):
                    lhs = scaled[:, start : start + mxu_width]
                    step(index, acc_in, [lhs] * mxus)
                    index += 1

            mean = jnp.sum(total, axis=-1, keepdims=True) / width
            square = jnp.sum(squares, axis=-1, keepdims=True) / width
            variance = jnp.maximum(square - mean * mean, 0.0)
            scale = jnp.where(section > 0, lax.rsqrt(variance + norm_eps), 1.0)
            lower = scale * mean

            @pl.when(entering & (section < last))
            def _():
                norm_send()

            projected = popped(acc_in) * scale - lower * folded[0] + folded[1]
            projected = projected.astype(jnp.bfloat16).astype(jnp.float32)
            projected = projected.reshape(pair, length, lru_width)
            tap_count = taps.shape[0]
            convolved = channel[0][None]
            for tap in range(tap_count):
                by = tap_count - 1 - tap
                shifted = delayed(projected, by, 0.0) if by else projected
                convolved = convolved + shifted * taps[tap : tap + 1][None]
            convolved = convolved.reshape(rows, lru_width).astype(jnp.bfloat16)
            lhs = [convolved[:, m * mxu_width : (m + 1) * mxu_width] for m in range(mxus)]
            pl.when(entering)(load_out[0].wait)
            step(index, acc_rate, lhs)
            step(index + 1, acc_input, lhs)
            index += 2
            for part in range(parts):
                raw = inbox[slot, :, :, across(part)].astype(jnp.float32).reshape(rows, -1)
                gain, shift = before[0, :, across(part)], before[1, :, across(part)]
                base[:, across(part)] = (raw * scale - lower) * gain + shift
            rate_gate = jax.nn.sigmoid(popped(acc_rate) + channel[1])
            input_gate = jax.nn.sigmoid(popped(acc_input) + channel[2])
            log_decay = rate_gate * channel[3]
            decay = jnp.exp(log_decay)
            scale_in = jnp.sqrt(-jnp.tanh(log_decay) * (decay * decay + 1.0))
            hidden = scale_in * input_gate * convolved.astype(jnp.float32)
            hidden = hidden.reshape(pair, length, lru_width)
            decay = decay.reshape(pair, length, lru_width)
            by = 1
            while by < length:
                hidden = decay * delayed(hidden, by, 0.0) + hidden
                if 2 * by < length:
                    decay = decay * delayed(decay, by, 1.0)
                by *= 2
            mixed = hidden.reshape(rows, lru_width).astype(jnp.bfloat16)

            def project(part):
                if part + 1 < parts:
                    pl.when(entering)(load_out[part + 1].wait)
                for k in range(mxus):
                    lhs = mixed[:, k * mxu_width : (k + 1) * mxu_width]
                    step(index + mxus * part + k, acc_out[part], [lhs] * mxus)

            def finish(part):
                away = base[:, across(part)] + popped(acc_out[part])
                outbox[slot, :, :, across(part)] = away.reshape(pair, length, -1).astype(
                    jnp.bfloat16
                )

                @pl.when(section < last)
                def _():
                    onward(slot, part).start()

                @pl.when((section == last) & (slot < last))
                def _():
                    home(slot, part, lead).start()

                for core_index in range(lead):
                    @pl.when(section == last)
                    def _():
                        home(slot, part, core_index).start()

            project(0)
            for part in range(1, parts):
                project(part)
                finish(part - 1)
            finish(parts - 1)

            return carry

        lax.fori_loop(0, sections, one_slot, 0)
        drain()

        @pl.when(section < last)
        def _():
            norm_onward.wait_send()
            for slot in range(sections):
                onward_all(slot).wait_send()

        @pl.when(section == last)
        def _():
            landing[...] = outbox[last, lead]
            for slot, core_index in homes:
                norm_home(slot, core_index).wait_send()
            for slot in range(last):
                homes_sent(slot, slice(0, pair)).wait_send()
            if lead:
                homes_sent(last, slice(0, lead)).wait_send()

    pairs = [accs[start : start + mxus] for start in range(0, len(accs), mxus)]

    @pl.when(leads)
    def _():
        run_section(pairs[0], pairs[1], pairs[2], pairs[3:])

    @pl.when(jnp.logical_not(first_stop))
    def _():
        pltpu.make_async_remote_copy(
            src_ref=tokens_hbm.at[0, 0],
            dst_ref=inbox.at[section, core],
            send_sem=entry_sem,
            recv_sem=recv_sem.at[section, 0],
            device_id=at(0, lead),
            device_id_type=MESH,
        ).wait_send()

    @pl.when(jnp.logical_not(last_stop))
    def _():
        pltpu.make_async_remote_copy(
            src_ref=norm,
            dst_ref=after,
            send_sem=entry_sem,
            recv_sem=norm_sem.at[2],
            device_id=at(0, lead),
            device_id_type=MESH,
        ).wait_recv()
        landed().wait_recv()

    raw = landing[...].astype(jnp.float32)
    mean = jnp.sum(fold_lanes(raw), axis=-1, keepdims=True) / width
    square = jnp.sum(fold_lanes(raw * raw), axis=-1, keepdims=True) / width
    variance = jnp.maximum(square - mean * mean, 0.0)
    scale = lax.rsqrt(variance + norm_eps)
    normed = (raw * scale - mean * scale) * after[0] + after[1]
    out_ref[0, 0] = normed.astype(jnp.bfloat16)


def shards(sections, pair, tokens_in, *weights):
    _, _, length, width = tokens_in.shape
    lru_width = weights[0].shape[2]
    tap_count = weights[1].shape[1]
    _, blocks, block_width, _ = weights[3].shape
    parts = width // (mxus * mxu_width)
    assert lru_width == mxus * mxu_width and mxu_width % block_width == 0
    vmem = pltpu.VMEM
    f32, bf16 = jnp.float32, jnp.bfloat16
    scoped = [
        pltpu.SemaphoreType.DMA((10 + 2 * parts,)),
        pltpu.SemaphoreType.DMA,
        pltpu.SemaphoreType.DMA((sections,)),
        pltpu.SemaphoreType.DMA((sections, parts)),
        pltpu.SemaphoreType.DMA,
        pltpu.SemaphoreType.DMA((3,)),
        pltpu.SemaphoreType.DMA((sections, pair)),
        pltpu.SemaphoreType.REGULAR,
        *[
            pltpu.ACC(mxu)((pair * length, mxu_width), jnp.float32)
            for _ in range(3 + parts)
            for mxu in range(mxus)
        ],
    ]

    def kernel(*refs):
        pl.run_scoped(functools.partial(stack_kernel, sections, *refs), *scoped)

    return pl.pallas_call(
        kernel,
        out_shape=pltpu.VMEM(tokens_in.shape, tokens_in.dtype),
        in_specs=[pl.BlockSpec(memory_space=pl.ANY)] * (1 + len(weights)),
        out_specs=pl.BlockSpec(memory_space=pltpu.VMEM),
        scratch_shapes=[
            vmem((width, lru_width), bf16),
            vmem((lru_width, width), bf16),
            vmem((tap_count, lru_width), f32),
            vmem((4, 1, lru_width), f32),
            vmem((2, blocks, block_width, block_width), bf16),
            vmem((2, 1, width), f32),
            vmem((2, 1, width), f32),
            vmem((2, 1, width), f32),
            vmem((length, width), bf16),
            vmem((2, mxus, mxu_width, mxu_width), bf16),
            vmem((2, 1, lru_width), f32),
            vmem((pair * length, width), f32),
            vmem((sections, pair, length, width), bf16),
            vmem((sections, pair, length, width), bf16),
        ],
        compiler_params=pltpu.CompilerParams(collective_id=0, has_side_effects=True),
        name="section_stack",
    )(tokens_in, *weights)


def solution(mesh):
    placed = (
        P("pp", ("fs", "tp"), None, None),
        P("pp", None, None),
        P("pp", None, None),
        P("pp", None),
        P("pp", None, None, None),
        P("pp", None),
        P("pp", None, None, None),
        P("pp", None),
        P("pp", None),
        P("pp", None, None),
        P("pp", None),
        P("pp", None),
    )
    pair = 2 if mesh.shape["tp"] % 2 == 0 else 1
    return jax.shard_map(
        functools.partial(shards, mesh.shape["pp"], pair),
        mesh=mesh,
        in_specs=placed,
        out_specs=P("pp", ("fs", "tp"), None, None),
        check_vma=False,
    )
```

```python
import functools

import jax
import jax.numpy as jnp
from jax import lax
from jax.experimental import pallas as pl
from jax.experimental.pallas import tpu as pltpu
from jax.sharding import PartitionSpec as P

decay_scale = 8.0
norm_eps = 1e-05
mxu_width = 256
mxus = 2
lanes = 128
smallest = 1e-30
MESH = pl.DeviceIdType.MESH


def fold_lanes(x):
    total = x[:, :lanes]
    for start in range(lanes, x.shape[1], lanes):
        total = total + x[:, start : start + lanes]
    return total


def stack_kernel(
    sections,
    tokens_hbm,
    w_in_hbm,
    taps_hbm,
    cbias_hbm,
    grate_hbm,
    brate_hbm,
    ginput_hbm,
    binput_hbm,
    dparam_hbm,
    w_out_hbm,
    gain_hbm,
    shift_hbm,
    out_ref,
    w_in,
    w_out,
    taps,
    channel,
    gates,
    norm,
    before,
    after,
    landing,
    maps,
    folded,
    masked,
    base,
    inbox,
    outbox,
    load_sem,
    entry_sem,
    send_sem,
    recv_sem,
    final_sem,
    norm_sem,
    home_sem,
    ready_sem,
    *accs,
):
    section = lax.axis_index("pp")
    column = lax.axis_index("tp")
    last = sections - 1
    pair, length = inbox.shape[1:3]
    rows = pair * length
    width, lru_width = w_in.shape
    parts = recv_sem.shape[1]
    part_width = width // parts
    tiles_in = width // mxu_width
    core = lax.rem(column, pair)
    lead = pair - 1
    leads = core == lead
    first_stop = leads & (section == 0)
    last_stop = leads & (section == last)

    def at(stop, core_index):
        return {"pp": stop, "tp": column - core + core_index}

    def across(part):
        return slice(part * part_width, (part + 1) * part_width)

    barrier = pltpu.get_barrier_semaphore()

    def tell(stop, core_index):
        pl.semaphore_signal(
            barrier, inc=1, device_id=at(stop, core_index), device_id_type=MESH
        )

    def load(src, dst, index):
        return pltpu.make_async_copy(src, dst, load_sem.at[index])

    own = load(tokens_hbm.at[0, 0], inbox.at[0, lead], 0)
    small = [
        load(grate_hbm.at[0], gates.at[0], 1),
        load(ginput_hbm.at[0], gates.at[1], 2),
        load(taps_hbm.at[0], taps, 3),
        load(cbias_hbm, channel.at[0], 4),
        load(brate_hbm, channel.at[1], 5),
        load(binput_hbm, channel.at[2], 6),
        load(dparam_hbm, channel.at[3], 7),
        load(gain_hbm, norm.at[0], 8),
        load(shift_hbm, norm.at[1], 9),
    ]
    load_in = [
        load(w_in_hbm.at[0, across(part)], w_in.at[across(part)], 10 + part)
        for part in range(parts)
    ]
    load_out = [
        load(w_out_hbm.at[0, :, across(part)], w_out.at[:, across(part)], 10 + parts + part)
        for part in range(parts)
    ]

    @pl.when(first_stop)
    def _():
        for stop in reversed(range(sections)):
            for core_index in range(pair):
                if (stop, core_index) != (0, lead):
                    tell(stop, core_index)

    @pl.when(jnp.logical_not(first_stop | last_stop))
    def _():
        tell(last, lead)

    @pl.when(leads & (section > 0) & (section + 1 < last))
    def _():
        tell(section + 1, lead)

    heard = jnp.where(
        last_stop, sections * pair - 1, jnp.where(leads & (section > 1), 2, 1)
    ).astype(jnp.int32)

    def entry(part):
        return pltpu.make_async_remote_copy(
            src_ref=tokens_hbm.at[0, 0, :, across(part)],
            dst_ref=inbox.at[section, core, :, across(part)],
            send_sem=entry_sem,
            recv_sem=recv_sem.at[section, part],
            device_id=at(0, lead),
            device_id_type=MESH,
        )

    @pl.when(jnp.logical_not(first_stop))
    def _():
        pl.semaphore_wait(barrier, heard)
        for part in range(parts):
            entry(part).start()

    @pl.when(first_stop)
    def _():
        own.start()

    @pl.when(leads & (section > 0))
    def _():
        pl.semaphore_signal(
            ready_sem, inc=1, device_id=at(section - 1, lead), device_id_type=MESH
        )

    @pl.when(leads)
    def _():
        for copy in small[:3]:
            copy.start()
        for copy in load_in:
            copy.start()
        for copy in small[3:] + load_out:
            copy.start()

    def arrival(slot, part, cores):
        return pltpu.make_async_remote_copy(
            src_ref=outbox.at[slot, cores, :, across(part)],
            dst_ref=inbox.at[slot, cores, :, across(part)],
            send_sem=entry_sem,
            recv_sem=recv_sem.at[slot, part],
            device_id=at(0, lead),
            device_id_type=MESH,
        )

    def onward(slot, part):
        return pltpu.make_async_remote_copy(
            src_ref=outbox.at[slot, :, :, across(part)],
            dst_ref=inbox.at[slot, :, :, across(part)],
            send_sem=send_sem.at[slot],
            recv_sem=recv_sem.at[slot, part],
            device_id=at(jnp.minimum(section + 1, last), lead),
            device_id_type=MESH,
        )

    def onward_all(slot):
        return pltpu.make_async_remote_copy(
            src_ref=outbox.at[slot],
            dst_ref=inbox.at[slot],
            send_sem=send_sem.at[slot],
            recv_sem=recv_sem.at[slot, 0],
            device_id=at(jnp.minimum(section + 1, last), lead),
            device_id_type=MESH,
        )

    def home(slot, part, core_index):
        return pltpu.make_async_remote_copy(
            src_ref=outbox.at[slot, core_index, :, across(part)],
            dst_ref=landing.at[:, across(part)],
            send_sem=send_sem.at[slot],
            recv_sem=final_sem,
            device_id=at(slot, core_index),
            device_id_type=MESH,
        )

    def landed():
        return pltpu.make_async_remote_copy(
            src_ref=landing,
            dst_ref=landing,
            send_sem=entry_sem,
            recv_sem=final_sem,
            device_id=at(0, lead),
            device_id_type=MESH,
        )

    def norm_home(slot, core_index):
        return pltpu.make_async_remote_copy(
            src_ref=norm,
            dst_ref=after,
            send_sem=home_sem.at[slot, core_index],
            recv_sem=norm_sem.at[2],
            device_id=at(slot, core_index),
            device_id_type=MESH,
        )

    homes = [
        (slot, core_index)
        for slot in range(sections)
        for core_index in reversed(range(pair))
        if (slot, core_index) != (last, lead)
    ]

    def homes_sent(slot, cores):
        return pltpu.make_async_remote_copy(
            src_ref=outbox.at[slot, cores],
            dst_ref=inbox.at[slot, cores],
            send_sem=send_sem.at[slot],
            recv_sem=final_sem,
            device_id=at(slot, lead),
            device_id_type=MESH,
        )

    norm_onward = pltpu.make_async_remote_copy(
        src_ref=norm,
        dst_ref=before,
        send_sem=norm_sem.at[0],
        recv_sem=norm_sem.at[1],
        device_id=at(jnp.minimum(section + 1, last), lead),
        device_id_type=MESH,
    )

    def tile(ref, row, col):
        return ref[
            row * mxu_width : (row + 1) * mxu_width,
            col * mxu_width : (col + 1) * mxu_width,
        ]

    def unit(index, mxu):
        index = index % (tiles_in + 2 + mxus * parts)
        if index < tiles_in:
            return tile(w_in, index, mxu)
        index -= tiles_in
        if index < 2:
            return maps[index, mxu]
        index -= 2
        return tile(w_out, index % mxus, (index // mxus) * mxus + mxu)

    def stage(index, mxu):
        pltpu.matmul_push_rhs(unit(index, mxu), staging_register=index % 2, mxu_index=mxu)

    def multiply(index, accs, lhs):
        for mxu in range(mxus):
            pltpu.matmul_acc_lhs(accs[mxu], lhs[mxu], load_staged_rhs=index % 2)

    def step(index, accs, lhs):
        multiply(index, accs, lhs)
        for mxu in range(mxus):
            stage(index + 2, mxu)

    def popped(accs):
        return jnp.concatenate([pltpu.matmul_pop(acc) for acc in accs], axis=1)

    def run_section(acc_in, acc_rate, acc_input, acc_out):
        def drain():
            nothing = jnp.zeros((rows, mxu_width), jnp.bfloat16)
            for mxu in range(mxus):
                for register in range(2):
                    pltpu.matmul_acc_lhs(acc_in[mxu], nothing, load_staged_rhs=register)
            popped(acc_in)

        drain()
        for accs in (acc_rate, acc_input, *acc_out):
            popped(accs)
        _, blocks, block_width, _ = gates.shape
        group = mxu_width // block_width
        maps[...] = jnp.zeros_like(maps)
        for copy in small:
            copy.wait()

        def norm_send():
            pl.semaphore_wait(ready_sem, 1)
            norm_onward.start()

        pl.when((section > 0) & (section < last))(norm_send)

        for gate in range(2):
            for block in range(blocks):
                to = (block % group) * block_width
                maps[gate, block // group, to : to + block_width, to : to + block_width] = (
                    gates[gate, block] * 0.5
                )
        minus_decay = -channel[3]
        softplus = jnp.maximum(minus_decay, 0.0) + jnp.log1p(jnp.exp(-jnp.abs(minus_decay)))
        channel[3] = -0.5 * decay_scale * softplus
        channel[1] = 0.5 * channel[1]
        channel[2] = 0.5 * channel[2]
        position = lax.broadcasted_iota(jnp.int32, (length, lru_width), 0)
        tap_count = taps.shape[0]
        for tap in range(tap_count):
            masked[tap] = jnp.where(position >= tap_count - 1 - tap, taps[tap : tap + 1], 0.0)

        @pl.when(first_stop)
        def _():
            own.wait()
            load_in[0].wait()
            before[0] = jnp.ones_like(before[0])
            before[1] = jnp.zeros_like(before[1])
            folded[...] = jnp.zeros_like(folded)

        @pl.when(section > 0)
        def _():
            for copy in load_in + load_out:
                copy.wait()
            norm_onward.wait_recv()
            which = lax.broadcasted_iota(jnp.int32, (rows, mxu_width), 0)
            for k in range(tiles_in):
                cols = slice(k * mxu_width, (k + 1) * mxu_width)
                split = []
                for vector in range(2):
                    value = before[vector, :, cols]
                    high = value.astype(jnp.bfloat16).astype(jnp.float32)
                    split += [high, value - high]
                lhs = jnp.zeros((rows, mxu_width), jnp.float32)
                for row, value in enumerate(split):
                    lhs = jnp.where(which == row, value, lhs)
                lhs = lhs.astype(jnp.bfloat16)
                for mxu in range(mxus):
                    stage(k, mxu)
                    pltpu.matmul_acc_lhs(acc_in[mxu], lhs, load_staged_rhs=k % 2)
            result = popped(acc_in)
            folded[0] = result[0:1] + result[1:2]
            folded[1] = result[2:3] + result[3:4]
            before[1] = before[1] - jnp.mean(before[1])

        for mxu in range(mxus):
            stage(0, mxu)
            stage(1, mxu)
        @pl.when(section == last)
        def _():
            after[...] = norm[...]
            for slot, core_index in homes:
                norm_home(slot, core_index).start()

        def one_slot(slot, carry):
            entering = (section == 0) & (slot == 0)
            total = jnp.zeros((rows, lanes), jnp.float32)
            squares = jnp.zeros((rows, lanes), jnp.float32)
            index = 0
            for part in range(parts):
                @pl.when(jnp.logical_not(entering))
                def _():
                    arrival(slot, part, slice(0, pair)).wait_recv()

                if lead:
                    @pl.when(entering)
                    def _():
                        arrival(slot, part, slice(0, lead)).wait_recv()

                raw = inbox[slot, :, :, across(part)].astype(jnp.float32).reshape(rows, -1)
                total = total + fold_lanes(raw)
                squares = squares + fold_lanes(raw * raw)
                if part + 1 < parts:
                    pl.when(entering)(load_in[part + 1].wait)
                scaled = (raw * before[0, :, across(part)]).astype(jnp.bfloat16)
                for start in range(0, part_width, mxu_width):
                    lhs = scaled[:, start : start + mxu_width]
                    step(index, acc_in, [lhs] * mxus)
                    index += 1

            mean = jnp.sum(total, axis=-1, keepdims=True) / width
            square = jnp.sum(squares, axis=-1, keepdims=True) / width
            variance = jnp.maximum(square - mean * mean, 0.0)
            scale = jnp.where(section > 0, lax.rsqrt(variance + norm_eps), 1.0)
            lower = scale * mean

            @pl.when(entering)
            def _():
                pl.when(section < last)(norm_send)
                for copy in load_out[:2]:
                    copy.wait()

            projected = popped(acc_in) * scale - lower * folded[0] + folded[1]
            projected = projected.astype(jnp.bfloat16).astype(jnp.float32)
            projected = projected.reshape(pair, length, lru_width)
            convolved = channel[0][None] + projected * masked[tap_count - 1][None]
            for by in range(1, tap_count):
                delayed = pltpu.roll(projected, by, 1)
                convolved = convolved + delayed * masked[tap_count - 1 - by][None]
            convolved = convolved.reshape(rows, lru_width).astype(jnp.bfloat16)
            lhs = [convolved[:, m * mxu_width : (m + 1) * mxu_width] for m in range(mxus)]
            step(index, acc_rate, lhs)
            step(index + 1, acc_input, lhs)
            index += 2
            for part in range(parts):
                raw = inbox[slot, :, :, across(part)].astype(jnp.float32).reshape(rows, -1)
                gain, shift = before[0, :, across(part)], before[1, :, across(part)]
                base[:, across(part)] = (raw * scale - lower) * gain + shift
            rate = jnp.tanh(popped(acc_rate) + channel[1])
            log_decay = rate * channel[3] + channel[3]
            decay = jnp.exp(log_decay)
            gap = -jnp.tanh(log_decay) * (decay * decay + 1.0)
            scale_in = gap * lax.rsqrt(jnp.maximum(gap, smallest))
            half = 0.5 * convolved.astype(jnp.float32)
            gated = jnp.tanh(popped(acc_input) + channel[2]) * half + half
            hidden = (scale_in * gated).reshape(pair, length, lru_width)
            decay = jnp.where(
                position[None] >= 1, decay.reshape(pair, length, lru_width), 0.0
            )
            by = 1
            while by < length:
                hidden = decay * pltpu.roll(hidden, by, 1) + hidden
                if 2 * by < length:
                    decay = decay * pltpu.roll(decay, by, 1)
                by *= 2
            mixed = hidden.reshape(rows, lru_width).astype(jnp.bfloat16)

            def project(part):
                for k in range(mxus):
                    lhs = mixed[:, k * mxu_width : (k + 1) * mxu_width]
                    multiply(index + mxus * part + k, acc_out[part], [lhs] * mxus)

            def prepare(part):
                for k in range(2):
                    for mxu in range(mxus):
                        stage(index + mxus * part + k, mxu)

            def finish(part):
                away = base[:, across(part)] + popped(acc_out[part])
                outbox[slot, :, :, across(part)] = away.reshape(pair, length, -1).astype(
                    jnp.bfloat16
                )

                @pl.when(section < last)
                def _():
                    onward(slot, part).start()

                @pl.when((section == last) & (slot < last))
                def _():
                    home(slot, part, lead).start()

                for core_index in range(lead):
                    @pl.when(section == last)
                    def _():
                        home(slot, part, core_index).start()

            project(0)
            for part in range(1, parts):
                prepare(part)
                project(part)
                finish(part - 1)
                if part == 1:
                    for copy in load_out[2:]:
                        pl.when(entering)(copy.wait)
            prepare(parts)
            finish(parts - 1)

            return carry

        lax.fori_loop(0, sections, one_slot, 0)
        drain()

        @pl.when(section < last)
        def _():
            norm_onward.wait_send()
            for slot in range(sections):
                onward_all(slot).wait_send()

        @pl.when(section == last)
        def _():
            landing[...] = outbox[last, lead]
            for slot, core_index in homes:
                norm_home(slot, core_index).wait_send()
            for slot in range(last):
                homes_sent(slot, slice(0, pair)).wait_send()
            if lead:
                homes_sent(last, slice(0, lead)).wait_send()

    pairs = [accs[start : start + mxus] for start in range(0, len(accs), mxus)]

    @pl.when(leads)
    def _():
        run_section(pairs[0], pairs[1], pairs[2], pairs[3:])

    @pl.when(jnp.logical_not(first_stop))
    def _():
        pltpu.make_async_remote_copy(
            src_ref=tokens_hbm.at[0, 0],
            dst_ref=inbox.at[section, core],
            send_sem=entry_sem,
            recv_sem=recv_sem.at[section, 0],
            device_id=at(0, lead),
            device_id_type=MESH,
        ).wait_send()

    @pl.when(jnp.logical_not(last_stop))
    def _():
        pltpu.make_async_remote_copy(
            src_ref=norm,
            dst_ref=after,
            send_sem=entry_sem,
            recv_sem=norm_sem.at[2],
            device_id=at(0, lead),
            device_id_type=MESH,
        ).wait_recv()
        landed().wait_recv()

    raw = landing[...].astype(jnp.float32)
    mean = jnp.sum(fold_lanes(raw), axis=-1, keepdims=True) / width
    square = jnp.sum(fold_lanes(raw * raw), axis=-1, keepdims=True) / width
    variance = jnp.maximum(square - mean * mean, 0.0)
    scale = lax.rsqrt(variance + norm_eps)
    normed = (raw * scale - mean * scale) * after[0] + after[1]
    out_ref[0, 0] = normed.astype(jnp.bfloat16)


def shards(sections, pair, tokens_in, *weights):
    _, _, length, width = tokens_in.shape
    lru_width = weights[0].shape[2]
    tap_count = weights[1].shape[1]
    _, blocks, block_width, _ = weights[3].shape
    parts = width // (mxus * mxu_width)
    assert lru_width == mxus * mxu_width and mxu_width % block_width == 0
    vmem = pltpu.VMEM
    f32, bf16 = jnp.float32, jnp.bfloat16
    scoped = [
        pltpu.SemaphoreType.DMA((10 + 2 * parts,)),
        pltpu.SemaphoreType.DMA,
        pltpu.SemaphoreType.DMA((sections,)),
        pltpu.SemaphoreType.DMA((sections, parts)),
        pltpu.SemaphoreType.DMA,
        pltpu.SemaphoreType.DMA((3,)),
        pltpu.SemaphoreType.DMA((sections, pair)),
        pltpu.SemaphoreType.REGULAR,
        *[
            pltpu.ACC(mxu)((pair * length, mxu_width), jnp.float32)
            for _ in range(3 + parts)
            for mxu in range(mxus)
        ],
    ]

    def kernel(*refs):
        pl.run_scoped(functools.partial(stack_kernel, sections, *refs), *scoped)

    return pl.pallas_call(
        kernel,
        out_shape=pltpu.VMEM(tokens_in.shape, tokens_in.dtype),
        in_specs=[pl.BlockSpec(memory_space=pl.ANY)] * (1 + len(weights)),
        out_specs=pl.BlockSpec(memory_space=pltpu.VMEM),
        scratch_shapes=[
            vmem((width, lru_width), bf16),
            vmem((lru_width, width), bf16),
            vmem((tap_count, lru_width), f32),
            vmem((4, 1, lru_width), f32),
            vmem((2, blocks, block_width, block_width), bf16),
            vmem((2, 1, width), f32),
            vmem((2, 1, width), f32),
            vmem((2, 1, width), f32),
            vmem((length, width), bf16),
            vmem((2, mxus, mxu_width, mxu_width), bf16),
            vmem((2, 1, lru_width), f32),
            vmem((tap_count, length, lru_width), f32),
            vmem((pair * length, width), f32),
            vmem((sections, pair, length, width), bf16),
            vmem((sections, pair, length, width), bf16),
        ],
        compiler_params=pltpu.CompilerParams(collective_id=0, has_side_effects=True),
        name="section_stack",
    )(tokens_in, *weights)


def solution(mesh):
    placed = (
        P("pp", ("fs", "tp"), None, None),
        P("pp", None, None),
        P("pp", None, None),
        P("pp", None),
        P("pp", None, None, None),
        P("pp", None),
        P("pp", None, None, None),
        P("pp", None),
        P("pp", None),
        P("pp", None, None),
        P("pp", None),
        P("pp", None),
    )
    pair = 2 if mesh.shape["tp"] % 2 == 0 else 1
    return jax.shard_map(
        functools.partial(shards, mesh.shape["pp"], pair),
        mesh=mesh,
        in_specs=placed,
        out_specs=P("pp", ("fs", "tp"), None, None),
        check_vma=False,
    )
```

```python
import functools

import jax
import jax.numpy as jnp
from jax import lax
from jax.experimental import pallas as pl
from jax.experimental.pallas import tpu as pltpu
from jax.sharding import PartitionSpec as P

decay_scale = 8.0
norm_eps = 1e-05
mxu_width = 256
mxus = 2
lanes = 128
smallest = 1e-30
log2_e = 1.4426950408889634
MESH = pl.DeviceIdType.MESH


def fold_lanes(x):
    total = x[:, :lanes]
    for start in range(lanes, x.shape[1], lanes):
        total = total + x[:, start : start + lanes]
    return total


def stack_kernel(
    sections,
    tokens_hbm,
    w_in_hbm,
    taps_hbm,
    cbias_hbm,
    grate_hbm,
    brate_hbm,
    ginput_hbm,
    binput_hbm,
    dparam_hbm,
    w_out_hbm,
    gain_hbm,
    shift_hbm,
    out_ref,
    w_in,
    w_out,
    taps,
    channel,
    gates,
    norm,
    before,
    after,
    landing,
    maps,
    folded,
    masked,
    base,
    inbox,
    outbox,
    load_sem,
    entry_sem,
    send_sem,
    recv_sem,
    final_sem,
    norm_sem,
    home_sem,
    ready_sem,
    *accs,
):
    section = lax.axis_index("pp")
    column = lax.axis_index("tp")
    last = sections - 1
    pair, length = inbox.shape[1:3]
    rows = pair * length
    width, lru_width = w_in.shape
    parts = recv_sem.shape[2]
    part_width = width // parts
    tiles_in = width // mxu_width
    core = lax.rem(column, pair)
    lead = pair - 1
    leads = core == lead
    first_stop = leads & (section == 0)
    last_stop = leads & (section == last)

    def at(stop, core_index):
        return {"pp": stop, "tp": column - core + core_index}

    def across(part):
        return slice(part * part_width, (part + 1) * part_width)

    barrier = pltpu.get_barrier_semaphore()

    def tell(stop, core_index):
        pl.semaphore_signal(
            barrier, inc=1, device_id=at(stop, core_index), device_id_type=MESH
        )

    def load(src, dst, index):
        return pltpu.make_async_copy(src, dst, load_sem.at[index])

    own = load(tokens_hbm.at[0, 0], inbox.at[0, lead], 0)
    small = [
        load(grate_hbm.at[0], gates.at[0], 1),
        load(ginput_hbm.at[0], gates.at[1], 2),
        load(taps_hbm.at[0], taps, 3),
        load(cbias_hbm, channel.at[0], 4),
        load(brate_hbm, channel.at[1], 5),
        load(binput_hbm, channel.at[2], 6),
        load(dparam_hbm, channel.at[3], 7),
        load(gain_hbm, norm.at[0], 8),
        load(shift_hbm, norm.at[1], 9),
    ]
    load_in = [
        load(w_in_hbm.at[0, across(part)], w_in.at[across(part)], 10 + part)
        for part in range(parts)
    ]
    load_out = [
        load(w_out_hbm.at[0, :, across(part)], w_out.at[:, across(part)], 10 + parts + part)
        for part in range(parts)
    ]

    @pl.when(first_stop)
    def _():
        for stop in reversed(range(sections)):
            for core_index in range(pair):
                if (stop, core_index) != (0, lead):
                    tell(stop, core_index)

    @pl.when(jnp.logical_not(first_stop | last_stop))
    def _():
        tell(last, lead)

    @pl.when(leads & (section > 0) & (section + 1 < last))
    def _():
        tell(section + 1, lead)

    heard = jnp.where(
        last_stop, sections * pair - 1, jnp.where(leads & (section > 1), 2, 1)
    ).astype(jnp.int32)

    def entry(part):
        return pltpu.make_async_remote_copy(
            src_ref=tokens_hbm.at[0, 0, :, across(part)],
            dst_ref=inbox.at[section, core, :, across(part)],
            send_sem=entry_sem,
            recv_sem=recv_sem.at[section, 0, part],
            device_id=at(0, lead),
            device_id_type=MESH,
        )

    @pl.when(jnp.logical_not(first_stop))
    def _():
        pl.semaphore_wait(barrier, heard)
        for part in range(parts):
            entry(part).start()

    @pl.when(first_stop)
    def _():
        own.start()

    @pl.when(leads & (section > 0))
    def _():
        pl.semaphore_signal(
            ready_sem, inc=1, device_id=at(section - 1, lead), device_id_type=MESH
        )

    @pl.when(leads)
    def _():
        for copy in small + load_in + load_out:
            copy.start()

    def onward(slot, first, count, part):
        cores = pl.ds(first, count)
        return pltpu.make_async_remote_copy(
            src_ref=outbox.at[slot, cores, :, across(part)],
            dst_ref=inbox.at[slot, cores, :, across(part)],
            send_sem=send_sem.at[slot],
            recv_sem=recv_sem.at[slot, first, part],
            device_id=at(jnp.minimum(section + 1, last), lead),
            device_id_type=MESH,
        )

    def onward_all(slot):
        return pltpu.make_async_remote_copy(
            src_ref=outbox.at[slot],
            dst_ref=inbox.at[slot],
            send_sem=send_sem.at[slot],
            recv_sem=recv_sem.at[slot, 0, 0],
            device_id=at(jnp.minimum(section + 1, last), lead),
            device_id_type=MESH,
        )

    def home(slot, core_index, part):
        return pltpu.make_async_remote_copy(
            src_ref=outbox.at[slot, core_index, :, across(part)],
            dst_ref=landing.at[:, across(part)],
            send_sem=send_sem.at[slot],
            recv_sem=final_sem,
            device_id=at(slot, core_index),
            device_id_type=MESH,
        )

    def landed():
        return pltpu.make_async_remote_copy(
            src_ref=landing,
            dst_ref=landing,
            send_sem=entry_sem,
            recv_sem=final_sem,
            device_id=at(0, lead),
            device_id_type=MESH,
        )

    def norm_home(slot, core_index):
        return pltpu.make_async_remote_copy(
            src_ref=norm,
            dst_ref=after,
            send_sem=home_sem.at[slot, core_index],
            recv_sem=norm_sem.at[2],
            device_id=at(slot, core_index),
            device_id_type=MESH,
        )

    homes = [
        (slot, core_index)
        for slot in range(sections)
        for core_index in reversed(range(pair))
        if (slot, core_index) != (last, lead)
    ]

    def homes_sent(slot, cores):
        return pltpu.make_async_remote_copy(
            src_ref=outbox.at[slot, cores],
            dst_ref=inbox.at[slot, cores],
            send_sem=send_sem.at[slot],
            recv_sem=final_sem,
            device_id=at(slot, lead),
            device_id_type=MESH,
        )

    norm_onward = pltpu.make_async_remote_copy(
        src_ref=norm,
        dst_ref=before,
        send_sem=norm_sem.at[0],
        recv_sem=norm_sem.at[1],
        device_id=at(jnp.minimum(section + 1, last), lead),
        device_id_type=MESH,
    )

    def tile(ref, row, col):
        return ref[
            row * mxu_width : (row + 1) * mxu_width,
            col * mxu_width : (col + 1) * mxu_width,
        ]

    def unit(index, mxu):
        index = index % (tiles_in + 2 + mxus * parts)
        if index < tiles_in:
            return tile(w_in, index, mxu)
        index -= tiles_in
        if index < 2:
            return maps[index, mxu]
        index -= 2
        return tile(w_out, index % mxus, (index // mxus) * mxus + mxu)

    def stage(index, mxu):
        pltpu.matmul_push_rhs(unit(index, mxu), staging_register=index % 2, mxu_index=mxu)

    def multiply(index, accs, lhs):
        for mxu in range(mxus):
            pltpu.matmul_acc_lhs(accs[mxu], lhs[mxu], load_staged_rhs=index % 2)

    def step(index, accs, lhs):
        multiply(index, accs, lhs)
        for mxu in range(mxus):
            stage(index + 2, mxu)

    def popped(accs):
        return jnp.concatenate([pltpu.matmul_pop(acc) for acc in accs], axis=1)

    def run_section(accs):
        def drain():
            nothing = jnp.zeros((rows, mxu_width), jnp.float32)
            for mxu in range(mxus):
                for register in range(2):
                    pltpu.matmul_acc_lhs(accs[0][mxu], nothing, load_staged_rhs=register)
            popped(accs[0])

        drain()
        for acc in accs[1:]:
            popped(acc)
        _, blocks, block_width, _ = gates.shape
        group = mxu_width // block_width
        maps[...] = jnp.zeros_like(maps)
        for copy in small:
            copy.wait()

        def norm_send():
            pl.semaphore_wait(ready_sem, 1)
            norm_onward.start()

        pl.when((section > 0) & (section < last))(norm_send)

        for gate in range(2):
            for block in range(blocks):
                to = (block % group) * block_width
                maps[gate, block // group, to : to + block_width, to : to + block_width] = (
                    gates[gate, block] * 0.5
                )
        minus_decay = -channel[3]
        softplus = jnp.maximum(minus_decay, 0.0) + jnp.log1p(jnp.exp(-jnp.abs(minus_decay)))
        channel[3] = 0.5 * decay_scale * softplus
        channel[1] = 0.5 * channel[1]
        channel[2] = 0.5 * channel[2]
        position = lax.broadcasted_iota(jnp.int32, (length, lru_width), 0)
        tap_count = taps.shape[0]
        for tap in range(tap_count):
            masked[tap] = jnp.where(position >= tap_count - 1 - tap, taps[tap : tap + 1], 0.0)

        @pl.when(first_stop)
        def _():
            own.wait()
            load_in[0].wait()
            before[0] = jnp.ones_like(before[0])
            before[1] = jnp.zeros_like(before[1])
            folded[...] = jnp.zeros_like(folded)

        @pl.when(section > 0)
        def _():
            for copy in load_in + load_out:
                copy.wait()
            norm_onward.wait_recv()
            which = lax.broadcasted_iota(jnp.int32, (rows, mxu_width), 0)
            for k in range(tiles_in):
                cols = slice(k * mxu_width, (k + 1) * mxu_width)
                split = []
                for vector in range(2):
                    value = before[vector, :, cols]
                    high = value.astype(jnp.bfloat16).astype(jnp.float32)
                    split += [high, value - high]
                lhs = jnp.zeros((rows, mxu_width), jnp.float32)
                for row, value in enumerate(split):
                    lhs = jnp.where(which == row, value, lhs)
                for mxu in range(mxus):
                    stage(k, mxu)
                    pltpu.matmul_acc_lhs(accs[0][mxu], lhs, load_staged_rhs=k % 2)
            result = popped(accs[0])
            folded[0] = result[0:1] + result[1:2]
            folded[1] = result[2:3] + result[3:4]
            before[1] = before[1] - jnp.mean(before[1])

        for mxu in range(mxus):
            stage(0, mxu)
            stage(1, mxu)
        @pl.when(section == last)
        def _():
            after[...] = norm[...]
            for slot, core_index in homes:
                norm_home(slot, core_index).start()

        def unit_of(slot, first, count, accs, opening):
            acc_in, acc_rate, acc_input, *acc_out = accs
            flat, deep = (count * length, -1), (count, length, -1)
            cores = pl.ds(first, count)

            def received(part):
                raw = inbox[slot, cores, :, across(part)]
                return raw.astype(jnp.float32).reshape(flat)

            def early(*copies):
                if opening:
                    @pl.when(section == 0)
                    def _():
                        for copy in copies:
                            copy.wait()

            total = jnp.zeros((count * length, lanes), jnp.float32)
            squares = jnp.zeros((count * length, lanes), jnp.float32)
            index = 0
            for part in range(parts):
                if opening:
                    @pl.when(section > 0)
                    def _():
                        onward(slot, first, count, part).wait_recv()

                    for other in range(lead):
                        @pl.when(section == 0)
                        def _():
                            onward(slot, other, 1, part).wait_recv()

                    early(*load_in[part + 1 : part + 2])
                else:
                    onward(slot, first, count, part).wait_recv()
                raw = received(part)
                total = total + fold_lanes(raw)
                squares = squares + fold_lanes(raw * raw)
                scaled = (raw * before[0, :, across(part)]).astype(jnp.bfloat16)
                for start in range(0, part_width, mxu_width):
                    lhs = scaled[:, start : start + mxu_width]
                    step(index, acc_in, [lhs] * mxus)
                    index += 1
            mean = jnp.sum(total, axis=-1, keepdims=True) / width
            square = jnp.sum(squares, axis=-1, keepdims=True) / width
            variance = jnp.maximum(square - mean * mean, 0.0)
            scale = jnp.where(section > 0, lax.rsqrt(variance + norm_eps), 1.0)
            lower = scale * mean
            constant = folded[1] - lower * folded[0]
            projected = popped(acc_in) * scale + constant
            projected = projected.reshape(deep)
            convolved = channel[0] + projected * masked[tap_count - 1]
            for by in range(1, tap_count):
                delayed = pltpu.roll(projected, by, 1)
                convolved = convolved + delayed * masked[tap_count - 1 - by]
            convolved = convolved.reshape(flat)
            rounded = convolved.astype(jnp.bfloat16)
            lhs = [rounded[:, m * mxu_width : (m + 1) * mxu_width] for m in range(mxus)]
            early(load_out[0])
            step(index, acc_rate, lhs)
            step(index + 1, acc_input, lhs)
            index += 2
            for part in range(parts):
                gain, shift = before[0, :, across(part)], before[1, :, across(part)]
                base[: count * length, across(part)] = (
                    received(part) * scale - lower
                ) * gain + shift
            rate = jnp.tanh(popped(acc_rate) + channel[1])
            fall = rate * channel[3] + channel[3]
            decay = jnp.exp2(fall * -log2_e)
            gap = jnp.tanh(fall) * (decay * decay + 1.0)
            scale_in = gap * lax.rsqrt(jnp.maximum(gap, smallest))
            half = 0.5 * convolved
            gated = jnp.tanh(popped(acc_input) + channel[2]) * half + half
            hidden = (scale_in * gated).reshape(deep)
            decay = jnp.where(position >= 1, decay.reshape(deep), 0.0)
            by = 1
            while by < length:
                hidden = decay * pltpu.roll(hidden, by, 1) + hidden
                if 2 * by < length:
                    decay = decay * pltpu.roll(decay, by, 1)
                by *= 2
            mixed = hidden.reshape(flat).astype(jnp.bfloat16)

            def project(part):
                for k in range(mxus):
                    lhs = mixed[:, k * mxu_width : (k + 1) * mxu_width]
                    multiply(index + mxus * part + k, acc_out[part], [lhs] * mxus)

            def prepare(part):
                for k in range(2):
                    for mxu in range(mxus):
                        stage(index + mxus * part + k, mxu)

            def finish(part):
                away = base[: count * length, across(part)] + popped(acc_out[part])
                outbox[slot, cores, :, across(part)] = away.reshape(deep).astype(jnp.bfloat16)

                @pl.when(section < last)
                def _():
                    onward(slot, first, count, part).start()

                @pl.when((section == last) & (slot < last))
                def _():
                    home(slot, lead, part).start()

                held = range(part - 1, part + 1) if part == parts - 1 else [part]
                for core_index in range(lead if part != parts - 2 else 0):
                    for ready_part in held:
                        @pl.when(section == last)
                        def _():
                            home(slot, core_index, ready_part).start()

            early(load_out[1])
            project(0)
            prepare(1)
            project(1)
            if opening:
                pl.when((section == 0) & (section < last))(norm_send)
            finish(0)
            early(*load_out[2:])
            for part in range(2, parts):
                prepare(part)
                project(part)
                if part < parts - 1:
                    finish(part - 1)
            prepare(parts)
            finish(parts - 2)
            finish(parts - 1)

        unit_of(0, 0, pair, accs, True)

        def one_slot(slot, carry):
            unit_of(slot, 0, pair, accs, False)
            return carry

        lax.fori_loop(1, sections, one_slot, 0)
        drain()

        @pl.when(section < last)
        def _():
            norm_onward.wait_send()
            for slot in range(sections):
                onward_all(slot).wait_send()

        @pl.when(section == last)
        def _():
            landing[...] = outbox[last, lead]
            for slot, core_index in homes:
                norm_home(slot, core_index).wait_send()
            for slot in range(last):
                homes_sent(slot, slice(0, pair)).wait_send()
            if lead:
                homes_sent(last, slice(0, lead)).wait_send()

    pairs = [accs[start : start + mxus] for start in range(0, len(accs), mxus)]

    @pl.when(leads)
    def _():
        run_section(pairs)

    @pl.when(jnp.logical_not(first_stop))
    def _():
        pltpu.make_async_remote_copy(
            src_ref=tokens_hbm.at[0, 0],
            dst_ref=inbox.at[section, core],
            send_sem=entry_sem,
            recv_sem=recv_sem.at[section, 0, 0],
            device_id=at(0, lead),
            device_id_type=MESH,
        ).wait_send()

    @pl.when(jnp.logical_not(last_stop))
    def _():
        pltpu.make_async_remote_copy(
            src_ref=norm,
            dst_ref=after,
            send_sem=entry_sem,
            recv_sem=norm_sem.at[2],
            device_id=at(0, lead),
            device_id_type=MESH,
        ).wait_recv()
        landed().wait_recv()

    raw = landing[...].astype(jnp.float32)
    mean = jnp.sum(fold_lanes(raw), axis=-1, keepdims=True) / width
    square = jnp.sum(fold_lanes(raw * raw), axis=-1, keepdims=True) / width
    variance = jnp.maximum(square - mean * mean, 0.0)
    scale = lax.rsqrt(variance + norm_eps)
    normed = (raw * scale - mean * scale) * after[0] + after[1]
    out_ref[0, 0] = normed.astype(jnp.bfloat16)


def shards(sections, pair, tokens_in, *weights):
    _, _, length, width = tokens_in.shape
    lru_width = weights[0].shape[2]
    tap_count = weights[1].shape[1]
    _, blocks, block_width, _ = weights[3].shape
    parts = width // (mxus * mxu_width)
    assert lru_width == mxus * mxu_width and mxu_width % block_width == 0
    vmem = pltpu.VMEM
    f32, bf16 = jnp.float32, jnp.bfloat16
    scoped = [
        pltpu.SemaphoreType.DMA((10 + 2 * parts,)),
        pltpu.SemaphoreType.DMA,
        pltpu.SemaphoreType.DMA((sections,)),
        pltpu.SemaphoreType.DMA((sections, pair, parts)),
        pltpu.SemaphoreType.DMA,
        pltpu.SemaphoreType.DMA((3,)),
        pltpu.SemaphoreType.DMA((sections, pair)),
        pltpu.SemaphoreType.REGULAR,
        *[
            pltpu.ACC(mxu)((pair * length, mxu_width), jnp.float32)
            for _ in range(3 + parts)
            for mxu in range(mxus)
        ],
    ]

    def kernel(*refs):
        pl.run_scoped(functools.partial(stack_kernel, sections, *refs), *scoped)

    return pl.pallas_call(
        kernel,
        out_shape=pltpu.VMEM(tokens_in.shape, tokens_in.dtype),
        in_specs=[pl.BlockSpec(memory_space=pl.ANY)] * (1 + len(weights)),
        out_specs=pl.BlockSpec(memory_space=pltpu.VMEM),
        scratch_shapes=[
            vmem((width, lru_width), bf16),
            vmem((lru_width, width), bf16),
            vmem((tap_count, lru_width), f32),
            vmem((4, 1, lru_width), f32),
            vmem((2, blocks, block_width, block_width), bf16),
            vmem((2, 1, width), f32),
            vmem((2, 1, width), f32),
            vmem((2, 1, width), f32),
            vmem((length, width), bf16),
            vmem((2, mxus, mxu_width, mxu_width), bf16),
            vmem((2, 1, lru_width), f32),
            vmem((tap_count, length, lru_width), f32),
            vmem((pair * length, width), f32),
            vmem((sections, pair, length, width), bf16),
            vmem((sections, pair, length, width), bf16),
        ],
        compiler_params=pltpu.CompilerParams(collective_id=0, has_side_effects=True),
        name="section_stack",
    )(tokens_in, *weights)


def solution(mesh):
    placed = (
        P("pp", ("fs", "tp"), None, None),
        P("pp", None, None),
        P("pp", None, None),
        P("pp", None),
        P("pp", None, None, None),
        P("pp", None),
        P("pp", None, None, None),
        P("pp", None),
        P("pp", None),
        P("pp", None, None),
        P("pp", None),
        P("pp", None),
    )
    pair = 2 if mesh.shape["tp"] % 2 == 0 else 1
    return jax.shard_map(
        functools.partial(shards, mesh.shape["pp"], pair),
        mesh=mesh,
        in_specs=placed,
        out_specs=P("pp", ("fs", "tp"), None, None),
        check_vma=False,
    )
```

```python
import functools

import jax
import jax.numpy as jnp
from jax import lax
from jax.experimental import pallas as pl
from jax.experimental.pallas import tpu as pltpu
from jax.sharding import PartitionSpec as P

decay_scale = 8.0
norm_eps = 1e-05
mxu_width = 256
mxus = 2
lanes = 128
smallest = 1e-30
log2_e = 1.4426950408889634
MESH = pl.DeviceIdType.MESH


def fold_lanes(x):
    total = x[:, :lanes]
    for start in range(lanes, x.shape[1], lanes):
        total = total + x[:, start : start + lanes]
    return total


def stack_kernel(
    sections,
    tokens_hbm,
    w_in_hbm,
    taps_hbm,
    cbias_hbm,
    grate_hbm,
    brate_hbm,
    ginput_hbm,
    binput_hbm,
    dparam_hbm,
    w_out_hbm,
    gain_hbm,
    shift_hbm,
    out_ref,
    w_in,
    w_out,
    taps,
    channel,
    gates,
    norm,
    before,
    after,
    landing,
    maps,
    folded,
    row_mean,
    masked,
    base,
    inbox,
    outbox,
    load_sem,
    entry_sem,
    send_sem,
    recv_sem,
    final_sem,
    norm_sem,
    home_sem,
    ready_sem,
    *accs,
):
    section = lax.axis_index("pp")
    column = lax.axis_index("tp")
    last = sections - 1
    pair, length = inbox.shape[1:3]
    rows = pair * length
    width, lru_width = w_in.shape
    parts = recv_sem.shape[2]
    part_width = width // parts
    tiles_in = width // mxu_width
    core = lax.rem(column, pair)
    lead = pair - 1
    leads = core == lead
    first_stop = leads & (section == 0)
    last_stop = leads & (section == last)

    def at(stop, core_index):
        return {"pp": stop, "tp": column - core + core_index}

    def across(part):
        return slice(part * part_width, (part + 1) * part_width)

    barrier = pltpu.get_barrier_semaphore()

    def tell(stop, core_index):
        pl.semaphore_signal(
            barrier, inc=1, device_id=at(stop, core_index), device_id_type=MESH
        )

    def load(src, dst, index):
        return pltpu.make_async_copy(src, dst, load_sem.at[index])

    own = load(tokens_hbm.at[0, 0], inbox.at[0, lead], 0)
    small = [
        load(grate_hbm.at[0], gates.at[0], 1),
        load(ginput_hbm.at[0], gates.at[1], 2),
        load(taps_hbm.at[0], taps, 3),
        load(cbias_hbm, channel.at[0], 4),
        load(brate_hbm, channel.at[1], 5),
        load(binput_hbm, channel.at[2], 6),
        load(dparam_hbm, channel.at[3], 7),
        load(gain_hbm, norm.at[0], 8),
        load(shift_hbm, norm.at[1], 9),
    ]
    load_in = [
        load(w_in_hbm.at[0, across(part)], w_in.at[across(part)], 10 + part)
        for part in range(parts)
    ]
    out_cols = [slice(0, mxu_width), slice(mxu_width, part_width)]
    out_cols += [across(part) for part in range(1, parts)]
    load_out = [
        load(w_out_hbm.at[0, :, cols], w_out.at[:, cols], 10 + parts + index)
        for index, cols in enumerate(out_cols)
    ]

    @pl.when(first_stop)
    def _():
        for stop in reversed(range(sections)):
            for core_index in range(pair):
                if (stop, core_index) != (0, lead):
                    tell(stop, core_index)

    @pl.when(jnp.logical_not(first_stop | last_stop))
    def _():
        tell(last, lead)

    @pl.when(leads & (section > 0) & (section + 1 < last))
    def _():
        tell(section + 1, lead)

    heard = jnp.where(
        last_stop, sections * pair - 1, jnp.where(leads & (section > 1), 2, 1)
    ).astype(jnp.int32)

    def entry(part):
        return pltpu.make_async_remote_copy(
            src_ref=tokens_hbm.at[0, 0, :, across(part)],
            dst_ref=inbox.at[section, core, :, across(part)],
            send_sem=entry_sem,
            recv_sem=recv_sem.at[section, 0, part],
            device_id=at(0, lead),
            device_id_type=MESH,
        )

    @pl.when(jnp.logical_not(first_stop))
    def _():
        pl.semaphore_wait(barrier, heard)
        for part in range(parts):
            entry(part).start()

    @pl.when(first_stop)
    def _():
        own.start()

    @pl.when(leads & (section > 0))
    def _():
        pl.semaphore_signal(
            ready_sem, inc=1, device_id=at(section - 1, lead), device_id_type=MESH
        )

    @pl.when(leads)
    def _():
        for copy in small + load_in[:2] + load_out[:1] + load_in[2:] + load_out[1:]:
            copy.start()

    def onward(slot, first, count, part):
        cores = pl.ds(first, count)
        return pltpu.make_async_remote_copy(
            src_ref=outbox.at[slot, cores, :, across(part)],
            dst_ref=inbox.at[slot, cores, :, across(part)],
            send_sem=send_sem.at[slot],
            recv_sem=recv_sem.at[slot, first, part],
            device_id=at(jnp.minimum(section + 1, last), lead),
            device_id_type=MESH,
        )

    def onward_all(slot):
        return pltpu.make_async_remote_copy(
            src_ref=outbox.at[slot],
            dst_ref=inbox.at[slot],
            send_sem=send_sem.at[slot],
            recv_sem=recv_sem.at[slot, 0, 0],
            device_id=at(jnp.minimum(section + 1, last), lead),
            device_id_type=MESH,
        )

    def home(slot, core_index, part):
        return pltpu.make_async_remote_copy(
            src_ref=outbox.at[slot, core_index, :, across(part)],
            dst_ref=landing.at[:, across(part)],
            send_sem=send_sem.at[slot],
            recv_sem=final_sem,
            device_id=at(slot, core_index),
            device_id_type=MESH,
        )

    def landed():
        return pltpu.make_async_remote_copy(
            src_ref=landing,
            dst_ref=landing,
            send_sem=entry_sem,
            recv_sem=final_sem,
            device_id=at(0, lead),
            device_id_type=MESH,
        )

    def norm_home(slot, core_index):
        return pltpu.make_async_remote_copy(
            src_ref=norm,
            dst_ref=after,
            send_sem=home_sem.at[slot, core_index],
            recv_sem=norm_sem.at[2],
            device_id=at(slot, core_index),
            device_id_type=MESH,
        )

    homes = [
        (slot, core_index)
        for slot in range(sections)
        for core_index in reversed(range(pair))
        if (slot, core_index) != (last, lead)
    ]

    def homes_sent(slot, cores):
        return pltpu.make_async_remote_copy(
            src_ref=outbox.at[slot, cores],
            dst_ref=inbox.at[slot, cores],
            send_sem=send_sem.at[slot],
            recv_sem=final_sem,
            device_id=at(slot, lead),
            device_id_type=MESH,
        )

    norm_onward = pltpu.make_async_remote_copy(
        src_ref=norm,
        dst_ref=before,
        send_sem=norm_sem.at[0],
        recv_sem=norm_sem.at[1],
        device_id=at(jnp.minimum(section + 1, last), lead),
        device_id_type=MESH,
    )

    def tile(ref, row, col):
        return ref[
            row * mxu_width : (row + 1) * mxu_width,
            col * mxu_width : (col + 1) * mxu_width,
        ]

    def unit(index, mxu):
        index = index % (tiles_in + 2 + mxus * parts)
        if index < tiles_in:
            return tile(w_in, index, mxu)
        index -= tiles_in
        if index < 2:
            return maps[index, mxu]
        index -= 2
        return tile(w_out, index % mxus, (index // mxus) * mxus + mxu)

    def stage(index, mxu):
        pltpu.matmul_push_rhs(unit(index, mxu), staging_register=index % 2, mxu_index=mxu)

    def multiply(index, accs, lhs):
        for mxu in range(mxus):
            pltpu.matmul_acc_lhs(accs[mxu], lhs[mxu], load_staged_rhs=index % 2)

    def step(index, accs, lhs):
        multiply(index, accs, lhs)
        for mxu in range(mxus):
            stage(index + 2, mxu)

    def popped(accs):
        return jnp.concatenate([pltpu.matmul_pop(acc) for acc in accs], axis=1)

    def run_section(accs):
        def drain():
            nothing = jnp.zeros((rows, mxu_width), jnp.float32)
            for mxu in range(mxus):
                for register in range(2):
                    pltpu.matmul_acc_lhs(accs[0][mxu], nothing, load_staged_rhs=register)
            popped(accs[0])

        drain()
        for acc in accs[1:]:
            popped(acc)
        _, blocks, block_width, _ = gates.shape
        group = mxu_width // block_width
        maps[...] = jnp.zeros_like(maps)
        for copy in small:
            copy.wait()

        def norm_send():
            pl.semaphore_wait(ready_sem, 1)
            norm_onward.start()

        pl.when((section > 0) & (section < last))(norm_send)

        for gate in range(2):
            for block in range(blocks):
                to = (block % group) * block_width
                maps[gate, block // group, to : to + block_width, to : to + block_width] = (
                    gates[gate, block] * 0.5
                )
        minus_decay = -channel[3]
        softplus = jnp.maximum(minus_decay, 0.0) + jnp.log1p(jnp.exp(-jnp.abs(minus_decay)))
        channel[3] = 0.5 * decay_scale * softplus
        channel[1] = 0.5 * channel[1]
        channel[2] = 0.5 * channel[2]
        position = lax.broadcasted_iota(jnp.int32, (length, lru_width), 0)
        tap_count = taps.shape[0]
        for tap in range(tap_count):
            masked[tap] = jnp.where(position >= tap_count - 1 - tap, taps[tap : tap + 1], 0.0)

        def norm_rows(index):
            cols = slice(index * mxu_width, (index + 1) * mxu_width)
            which = lax.broadcasted_iota(jnp.int32, (rows, mxu_width), 0)
            lhs = jnp.zeros((rows, mxu_width), jnp.float32)
            for vector in range(2):
                value = before[vector, :, cols]
                high = value.astype(jnp.bfloat16).astype(jnp.float32)
                lhs = jnp.where(which == 2 * vector, high, lhs)
                lhs = jnp.where(which == 2 * vector + 1, value - high, lhs)
            return lhs.astype(jnp.bfloat16)

        def average(register):
            load_out[0].wait()
            ones = jnp.ones((rows, mxu_width), jnp.float32)
            for mxu in range(mxus):
                pltpu.matmul_push_rhs(
                    tile(w_out, mxu, 0),
                    staging_register=register,
                    mxu_index=mxu,
                    transpose=True,
                )
            multiply(register, accs[1], [ones] * mxus)

        @pl.when(first_stop)
        def _():
            own.wait()
            load_in[0].wait()
            folded[...] = jnp.zeros_like(folded)
            before[0] = jnp.ones_like(before[0])
            before[1] = jnp.zeros_like(before[1])

        @pl.when(section > 0)
        def _():
            average(0)
            for copy in load_in + load_out[1:]:
                copy.wait()
            norm_onward.wait_recv()
            for k in range(tiles_in):
                for mxu in range(mxus):
                    stage(k, mxu)
                multiply(k, accs[0], [norm_rows(k)] * mxus)
            result = popped(accs[0])
            folded[0] = result[0:1] + result[1:2]
            folded[1] = result[2:3] + result[3:4]

        for mxu in range(mxus):
            stage(0, mxu)
            stage(1, mxu)
        @pl.when(section == last)
        def _():
            after[...] = norm[...]
            for slot, core_index in homes:
                norm_home(slot, core_index).start()

        def unit_of(slot, first, count, accs, opening):
            acc_in, acc_rate, acc_input, *acc_out = accs
            flat, deep = (count * length, -1), (count, length, -1)
            cores = pl.ds(first, count)

            def received(part):
                raw = inbox[slot, cores, :, across(part)]
                return raw.astype(jnp.float32).reshape(flat)

            def early(*copies):
                if opening:
                    @pl.when(section == 0)
                    def _():
                        for copy in copies:
                            copy.wait()

            total = jnp.zeros((count * length, lanes), jnp.float32)
            squares = jnp.zeros((count * length, lanes), jnp.float32)
            index = 0
            for part in range(parts):
                if opening:
                    @pl.when(section > 0)
                    def _():
                        onward(slot, first, count, part).wait_recv()

                    for other in range(lead):
                        @pl.when(section == 0)
                        def _():
                            onward(slot, other, 1, part).wait_recv()

                    early(*load_in[part + 1 : part + 2])
                else:
                    onward(slot, first, count, part).wait_recv()
                raw = received(part)
                total = total + fold_lanes(raw)
                squares = squares + fold_lanes(raw * raw)
                scaled = (raw * before[0, :, across(part)]).astype(jnp.bfloat16)
                for start in range(0, part_width, mxu_width):
                    lhs = scaled[:, start : start + mxu_width]
                    multiply(index, acc_in, [lhs] * mxus)
                    if opening and index == tiles_in // 2 - 1:
                        pl.when(section == 0)(functools.partial(average, index % 2))
                    for mxu in range(mxus):
                        stage(index + 2, mxu)
                    index += 1
            if opening:
                row_mean[...] = popped(accs[1])[0:1] * (1.0 / mxu_width)
            mean = jnp.sum(total, axis=-1, keepdims=True) / width
            square = jnp.sum(squares, axis=-1, keepdims=True) / width
            variance = jnp.maximum(square - mean * mean, 0.0)
            scale = jnp.where(section > 0, lax.rsqrt(variance + norm_eps), 1.0)
            lower = scale * mean
            constant = folded[1] - lower * folded[0]
            projected = popped(acc_in) * scale + constant
            projected = projected.reshape(deep)
            convolved = channel[0] + projected * masked[tap_count - 1]
            for by in range(1, tap_count):
                delayed = pltpu.roll(projected, by, 1)
                convolved = convolved + delayed * masked[tap_count - 1 - by]
            convolved = convolved.reshape(flat)
            rounded = convolved.astype(jnp.bfloat16)
            lhs = [rounded[:, m * mxu_width : (m + 1) * mxu_width] for m in range(mxus)]
            early(load_out[1])
            step(index, acc_rate, lhs)
            step(index + 1, acc_input, lhs)
            index += 2
            for part in range(parts):
                gain, shift = before[0, :, across(part)], before[1, :, across(part)]
                stream = (received(part) * scale - lower) * gain + shift
                base[: count * length, across(part)] = stream
                if part == 0:
                    common = fold_lanes(stream[:, :mxu_width]) * (1.0 / mxu_width)
            rate = jnp.tanh(popped(acc_rate) + channel[1])
            fall = rate * channel[3] + channel[3]
            decay = jnp.exp2(fall * -log2_e)
            gap = jnp.tanh(fall) * (decay * decay + 1.0)
            scale_in = gap * lax.rsqrt(jnp.maximum(gap, smallest))
            half = 0.5 * convolved
            gated = jnp.tanh(popped(acc_input) + channel[2]) * half + half
            hidden = (scale_in * gated).reshape(deep)
            decay = jnp.where(position >= 1, decay.reshape(deep), 0.0)
            by = 1
            while by < length:
                hidden = decay * pltpu.roll(hidden, by, 1) + hidden
                if 2 * by < length:
                    decay = decay * pltpu.roll(decay, by, 1)
                by *= 2
            mixed = hidden.reshape(flat)
            common = common + fold_lanes(mixed * row_mean[...])
            common = jnp.sum(common, axis=-1, keepdims=True)
            mixed = mixed.astype(jnp.bfloat16)

            def project(part):
                for k in range(mxus):
                    lhs = mixed[:, k * mxu_width : (k + 1) * mxu_width]
                    multiply(index + mxus * part + k, acc_out[part], [lhs] * mxus)

            def prepare(part):
                for k in range(2):
                    for mxu in range(mxus):
                        stage(index + mxus * part + k, mxu)

            def finish(part):
                away = base[: count * length, across(part)] - common + popped(acc_out[part])
                outbox[slot, cores, :, across(part)] = away.reshape(deep).astype(jnp.bfloat16)

                @pl.when(section < last)
                def _():
                    onward(slot, first, count, part).start()

                ahead = [lead] if not opening else list(range(lead))
                behind = list(range(lead)) if not opening else [lead]
                held = range(part - 1, part + 1) if part == parts - 1 else [part]
                sends = [(core_index, part) for core_index in ahead]
                if part != parts - 2:
                    sends += [(core_index, late) for core_index in behind for late in held]
                for core_index, ready_part in sends:
                    @pl.when((section == last) & ((slot < last) | (core_index < lead)))
                    def _():
                        home(slot, core_index, ready_part).start()

            early(load_out[2])
            project(0)
            prepare(1)
            project(1)
            if opening:
                pl.when((section == 0) & (section < last))(norm_send)
            finish(0)
            early(*load_out[3:])
            for part in range(2, parts):
                prepare(part)
                project(part)
                if part < parts - 1:
                    finish(part - 1)
            prepare(parts)
            finish(parts - 2)
            finish(parts - 1)

        unit_of(0, 0, pair, accs, True)

        def one_slot(slot, carry):
            unit_of(slot, 0, pair, accs, False)
            return carry

        lax.fori_loop(1, sections, one_slot, 0)
        drain()

        @pl.when(section < last)
        def _():
            norm_onward.wait_send()
            for slot in range(sections):
                onward_all(slot).wait_send()

        @pl.when(section == last)
        def _():
            landing[...] = outbox[last, lead]
            for slot, core_index in homes:
                norm_home(slot, core_index).wait_send()
            for slot in range(last):
                homes_sent(slot, slice(0, pair)).wait_send()
            if lead:
                homes_sent(last, slice(0, lead)).wait_send()

    pairs = [accs[start : start + mxus] for start in range(0, len(accs), mxus)]

    @pl.when(leads)
    def _():
        run_section(pairs)

    @pl.when(jnp.logical_not(first_stop))
    def _():
        pltpu.make_async_remote_copy(
            src_ref=tokens_hbm.at[0, 0],
            dst_ref=inbox.at[section, core],
            send_sem=entry_sem,
            recv_sem=recv_sem.at[section, 0, 0],
            device_id=at(0, lead),
            device_id_type=MESH,
        ).wait_send()

    @pl.when(jnp.logical_not(last_stop))
    def _():
        pltpu.make_async_remote_copy(
            src_ref=norm,
            dst_ref=after,
            send_sem=entry_sem,
            recv_sem=norm_sem.at[2],
            device_id=at(0, lead),
            device_id_type=MESH,
        ).wait_recv()
        landed().wait_recv()

    raw = landing[...].astype(jnp.float32)
    mean = jnp.sum(fold_lanes(raw), axis=-1, keepdims=True) / width
    square = jnp.sum(fold_lanes(raw * raw), axis=-1, keepdims=True) / width
    variance = jnp.maximum(square - mean * mean, 0.0)
    scale = lax.rsqrt(variance + norm_eps)
    normed = (raw * scale - mean * scale) * after[0] + after[1]
    out_ref[0, 0] = normed.astype(jnp.bfloat16)


def shards(sections, pair, tokens_in, *weights):
    _, _, length, width = tokens_in.shape
    lru_width = weights[0].shape[2]
    tap_count = weights[1].shape[1]
    _, blocks, block_width, _ = weights[3].shape
    parts = width // (mxus * mxu_width)
    assert lru_width == mxus * mxu_width and mxu_width % block_width == 0
    vmem = pltpu.VMEM
    f32, bf16 = jnp.float32, jnp.bfloat16
    scoped = [
        pltpu.SemaphoreType.DMA((11 + 2 * parts,)),
        pltpu.SemaphoreType.DMA,
        pltpu.SemaphoreType.DMA((sections,)),
        pltpu.SemaphoreType.DMA((sections, pair, parts)),
        pltpu.SemaphoreType.DMA,
        pltpu.SemaphoreType.DMA((3,)),
        pltpu.SemaphoreType.DMA((sections, pair)),
        pltpu.SemaphoreType.REGULAR,
        *[
            pltpu.ACC(mxu)((pair * length, mxu_width), jnp.float32)
            for _ in range(3 + parts)
            for mxu in range(mxus)
        ],
    ]

    def kernel(*refs):
        pl.run_scoped(functools.partial(stack_kernel, sections, *refs), *scoped)

    return pl.pallas_call(
        kernel,
        out_shape=pltpu.VMEM(tokens_in.shape, tokens_in.dtype),
        in_specs=[pl.BlockSpec(memory_space=pl.ANY)] * (1 + len(weights)),
        out_specs=pl.BlockSpec(memory_space=pltpu.VMEM),
        scratch_shapes=[
            vmem((width, lru_width), bf16),
            vmem((lru_width, width), bf16),
            vmem((tap_count, lru_width), f32),
            vmem((4, 1, lru_width), f32),
            vmem((2, blocks, block_width, block_width), bf16),
            vmem((2, 1, width), f32),
            vmem((2, 1, width), f32),
            vmem((2, 1, width), f32),
            vmem((length, width), bf16),
            vmem((2, mxus, mxu_width, mxu_width), bf16),
            vmem((2, 1, lru_width), f32),
            vmem((1, lru_width), f32),
            vmem((tap_count, length, lru_width), f32),
            vmem((pair * length, width), f32),
            vmem((sections, pair, length, width), bf16),
            vmem((sections, pair, length, width), bf16),
        ],
        compiler_params=pltpu.CompilerParams(collective_id=0, has_side_effects=True),
        name="section_stack",
    )(tokens_in, *weights)


def solution(mesh):
    placed = (
        P("pp", ("fs", "tp"), None, None),
        P("pp", None, None),
        P("pp", None, None),
        P("pp", None),
        P("pp", None, None, None),
        P("pp", None),
        P("pp", None, None, None),
        P("pp", None),
        P("pp", None),
        P("pp", None, None),
        P("pp", None),
        P("pp", None),
    )
    pair = 2 if mesh.shape["tp"] % 2 == 0 else 1
    return jax.shard_map(
        functools.partial(shards, mesh.shape["pp"], pair),
        mesh=mesh,
        in_specs=placed,
        out_specs=P("pp", ("fs", "tp"), None, None),
        check_vma=False,
    )
```

```python
import functools

import jax
import jax.numpy as jnp
from jax import lax
from jax.experimental import pallas as pl
from jax.experimental.pallas import tpu as pltpu
from jax.sharding import PartitionSpec as P

decay_scale = 8.0
norm_eps = 1e-05
mxu_width = 256
mxus = 2
lanes = 128
smallest = 1e-30
log2_e = 1.4426950408889634
MESH = pl.DeviceIdType.MESH


def fold_lanes(x):
    total = x[:, :lanes]
    for start in range(lanes, x.shape[1], lanes):
        total = total + x[:, start : start + lanes]
    return total


def stack_kernel(
    sections,
    tokens_hbm,
    w_in_hbm,
    taps_hbm,
    cbias_hbm,
    grate_hbm,
    brate_hbm,
    ginput_hbm,
    binput_hbm,
    dparam_hbm,
    w_out_hbm,
    gain_hbm,
    shift_hbm,
    out_ref,
    w_in,
    w_out,
    taps,
    channel,
    gates,
    norm,
    before,
    after,
    landing,
    maps,
    folded,
    row_mean,
    masked,
    base,
    inbox,
    outbox,
    load_sem,
    entry_sem,
    send_sem,
    recv_sem,
    final_sem,
    norm_sem,
    home_sem,
    ready_sem,
    *accs,
):
    section = lax.axis_index("pp")
    column = lax.axis_index("tp")
    last = sections - 1
    pair, length = inbox.shape[1:3]
    rows = pair * length
    width, lru_width = w_in.shape
    parts = recv_sem.shape[2]
    part_width = width // parts
    tiles_in = width // mxu_width
    core = lax.rem(column, pair)
    lead = pair - 1
    leads = core == lead
    first_stop = leads & (section == 0)
    last_stop = leads & (section == last)

    def at(stop, core_index):
        return {"pp": stop, "tp": column - core + core_index}

    def across(part):
        return slice(part * part_width, (part + 1) * part_width)

    barrier = pltpu.get_barrier_semaphore()

    def tell(stop, core_index):
        pl.semaphore_signal(
            barrier, inc=1, device_id=at(stop, core_index), device_id_type=MESH
        )

    def load(src, dst, index):
        return pltpu.make_async_copy(src, dst, load_sem.at[index])

    own = load(tokens_hbm.at[0, 0], inbox.at[0, lead], 0)
    small = [
        load(grate_hbm.at[0], gates.at[0], 1),
        load(ginput_hbm.at[0], gates.at[1], 2),
        load(taps_hbm.at[0], taps, 3),
        load(cbias_hbm, channel.at[0], 4),
        load(brate_hbm, channel.at[1], 5),
        load(binput_hbm, channel.at[2], 6),
        load(dparam_hbm, channel.at[3], 7),
        load(gain_hbm, norm.at[0], 8),
        load(shift_hbm, norm.at[1], 9),
    ]
    load_in = [
        load(w_in_hbm.at[0, across(part)], w_in.at[across(part)], 10 + part)
        for part in range(parts)
    ]
    out_cols = [slice(0, mxu_width), slice(mxu_width, part_width)]
    out_cols += [across(part) for part in range(1, parts)]
    load_out = [
        load(w_out_hbm.at[0, :, cols], w_out.at[:, cols], 10 + parts + index)
        for index, cols in enumerate(out_cols)
    ]

    @pl.when(first_stop)
    def _():
        for stop in reversed(range(sections)):
            for core_index in range(pair):
                if (stop, core_index) != (0, lead):
                    tell(stop, core_index)

    @pl.when(jnp.logical_not(first_stop | last_stop))
    def _():
        tell(last, lead)

    @pl.when(leads & (section > 0) & (section + 1 < last))
    def _():
        tell(section + 1, lead)

    heard = jnp.where(
        last_stop, sections * pair - 1, jnp.where(leads & (section > 1), 2, 1)
    ).astype(jnp.int32)

    def entry(part):
        return pltpu.make_async_remote_copy(
            src_ref=tokens_hbm.at[0, 0, :, across(part)],
            dst_ref=inbox.at[section, core, :, across(part)],
            send_sem=entry_sem,
            recv_sem=recv_sem.at[section, 0, part],
            device_id=at(0, lead),
            device_id_type=MESH,
        )

    @pl.when(jnp.logical_not(first_stop))
    def _():
        pl.semaphore_wait(barrier, heard)
        for part in range(parts):
            entry(part).start()

    @pl.when(first_stop)
    def _():
        own.start()

    @pl.when(leads & (section > 0))
    def _():
        pl.semaphore_signal(
            ready_sem, inc=1, device_id=at(section - 1, lead), device_id_type=MESH
        )

    @pl.when(leads)
    def _():
        for copy in small + load_in[:2] + load_out[:1] + load_in[2:] + load_out[1:]:
            copy.start()

    def onward(slot, first, count, part):
        cores = pl.ds(first, count)
        return pltpu.make_async_remote_copy(
            src_ref=outbox.at[slot, cores, :, across(part)],
            dst_ref=inbox.at[slot, cores, :, across(part)],
            send_sem=send_sem.at[slot],
            recv_sem=recv_sem.at[slot, first, part],
            device_id=at(jnp.minimum(section + 1, last), lead),
            device_id_type=MESH,
        )

    def onward_all(slot):
        return pltpu.make_async_remote_copy(
            src_ref=outbox.at[slot],
            dst_ref=inbox.at[slot],
            send_sem=send_sem.at[slot],
            recv_sem=recv_sem.at[slot, 0, 0],
            device_id=at(jnp.minimum(section + 1, last), lead),
            device_id_type=MESH,
        )

    def home(slot, core_index, part):
        return pltpu.make_async_remote_copy(
            src_ref=outbox.at[slot, core_index, :, across(part)],
            dst_ref=landing.at[:, across(part)],
            send_sem=send_sem.at[slot],
            recv_sem=final_sem,
            device_id=at(slot, core_index),
            device_id_type=MESH,
        )

    def landed():
        return pltpu.make_async_remote_copy(
            src_ref=landing,
            dst_ref=landing,
            send_sem=entry_sem,
            recv_sem=final_sem,
            device_id=at(0, lead),
            device_id_type=MESH,
        )

    def norm_home(slot, core_index):
        return pltpu.make_async_remote_copy(
            src_ref=norm,
            dst_ref=after,
            send_sem=home_sem.at[slot, core_index],
            recv_sem=norm_sem.at[2],
            device_id=at(slot, core_index),
            device_id_type=MESH,
        )

    homes = [
        (slot, core_index)
        for slot in range(sections)
        for core_index in reversed(range(pair))
        if (slot, core_index) != (last, lead)
    ]

    def homes_sent(slot, cores):
        return pltpu.make_async_remote_copy(
            src_ref=outbox.at[slot, cores],
            dst_ref=inbox.at[slot, cores],
            send_sem=send_sem.at[slot],
            recv_sem=final_sem,
            device_id=at(slot, lead),
            device_id_type=MESH,
        )

    norm_onward = pltpu.make_async_remote_copy(
        src_ref=norm,
        dst_ref=before,
        send_sem=norm_sem.at[0],
        recv_sem=norm_sem.at[1],
        device_id=at(jnp.minimum(section + 1, last), lead),
        device_id_type=MESH,
    )

    def tile(ref, row, col):
        return ref[
            row * mxu_width : (row + 1) * mxu_width,
            col * mxu_width : (col + 1) * mxu_width,
        ]

    def unit(index, mxu):
        index = index % (tiles_in + 2 + mxus * parts)
        if index < tiles_in:
            return tile(w_in, index, mxu)
        index -= tiles_in
        if index < 2:
            return maps[index, mxu]
        index -= 2
        return tile(w_out, index % mxus, (index // mxus) * mxus + mxu)

    def stage(index, mxu):
        pltpu.matmul_push_rhs(unit(index, mxu), staging_register=index % 2, mxu_index=mxu)

    def multiply(index, accs, lhs):
        for mxu in range(mxus):
            pltpu.matmul_acc_lhs(accs[mxu], lhs[mxu], load_staged_rhs=index % 2)

    def step(index, accs, lhs):
        multiply(index, accs, lhs)
        for mxu in range(mxus):
            stage(index + 2, mxu)

    def popped(accs):
        return jnp.concatenate([pltpu.matmul_pop(acc) for acc in accs], axis=1)

    def run_section(accs):
        def drain():
            nothing = jnp.zeros((rows, mxu_width), jnp.float32)
            for mxu in range(mxus):
                for register in range(2):
                    pltpu.matmul_acc_lhs(accs[0][mxu], nothing, load_staged_rhs=register)
            popped(accs[0])

        drain()
        for acc in accs[1:]:
            popped(acc)
        _, blocks, block_width, _ = gates.shape
        group = mxu_width // block_width
        maps[...] = jnp.zeros_like(maps)
        for copy in small:
            copy.wait()

        def norm_send():
            pl.semaphore_wait(ready_sem, 1)
            norm_onward.start()

        pl.when((section > 0) & (section < last))(norm_send)

        for gate in range(2):
            for block in range(blocks):
                to = (block % group) * block_width
                maps[gate, block // group, to : to + block_width, to : to + block_width] = (
                    gates[gate, block] * 0.5
                )
        minus_decay = -channel[3]
        softplus = jnp.maximum(minus_decay, 0.0) + jnp.log1p(jnp.exp(-jnp.abs(minus_decay)))
        channel[3] = 0.5 * decay_scale * softplus
        channel[1] = 0.5 * channel[1]
        channel[2] = 0.5 * channel[2]
        position = lax.broadcasted_iota(jnp.int32, (length, lru_width), 0)
        tap_count = taps.shape[0]
        for tap in range(tap_count):
            masked[tap] = jnp.where(position >= tap_count - 1 - tap, taps[tap : tap + 1], 0.0)

        def norm_rows(index):
            cols = slice(index * mxu_width, (index + 1) * mxu_width)
            which = lax.broadcasted_iota(jnp.int32, (rows, mxu_width), 0)
            lhs = jnp.zeros((rows, mxu_width), jnp.float32)
            for vector in range(2):
                value = before[vector, :, cols]
                high = value.astype(jnp.bfloat16).astype(jnp.float32)
                lhs = jnp.where(which == 2 * vector, high, lhs)
                lhs = jnp.where(which == 2 * vector + 1, value - high, lhs)
            return lhs.astype(jnp.bfloat16)

        def average(register):
            load_out[0].wait()
            ones = jnp.ones((rows, mxu_width), jnp.float32)
            for mxu in range(mxus):
                pltpu.matmul_push_rhs(
                    tile(w_out, mxu, 0),
                    staging_register=register,
                    mxu_index=mxu,
                    transpose=True,
                )
            multiply(register, accs[1], [ones] * mxus)

        @pl.when(first_stop)
        def _():
            own.wait()
            load_in[0].wait()
            folded[...] = jnp.zeros_like(folded)
            before[0] = jnp.ones_like(before[0])
            before[1] = jnp.zeros_like(before[1])

        @pl.when(section > 0)
        def _():
            average(0)
            for copy in load_in + load_out[1:]:
                copy.wait()
            norm_onward.wait_recv()
            for k in range(tiles_in):
                for mxu in range(mxus):
                    stage(k, mxu)
                multiply(k, accs[0], [norm_rows(k)] * mxus)
            result = popped(accs[0])
            folded[0] = result[0:1] + result[1:2]
            folded[1] = result[2:3] + result[3:4]

        for mxu in range(mxus):
            stage(0, mxu)
            stage(1, mxu)
        @pl.when(section == last)
        def _():
            after[...] = norm[...]
            for slot, core_index in homes:
                norm_home(slot, core_index).start()

        def unit_of(slot, first, count, accs, opening):
            acc_in, acc_rate, acc_input, *acc_out = accs
            flat, deep = (count * length, -1), (count, length, -1)
            cores = pl.ds(first, count)

            def received(part):
                raw = inbox[slot, cores, :, across(part)]
                return raw.astype(jnp.float32).reshape(flat)

            def early(*copies):
                if opening:
                    @pl.when(section == 0)
                    def _():
                        for copy in copies:
                            copy.wait()

            total = jnp.zeros((count * length, lanes), jnp.float32)
            squares = jnp.zeros((count * length, lanes), jnp.float32)
            index = 0
            for part in range(parts):
                if opening:
                    @pl.when(section > 0)
                    def _():
                        onward(slot, first, count, part).wait_recv()

                    for other in range(lead):
                        @pl.when(section == 0)
                        def _():
                            onward(slot, other, 1, part).wait_recv()

                    early(*load_in[part + 1 : part + 2])
                else:
                    onward(slot, first, count, part).wait_recv()
                raw = received(part)
                total = total + fold_lanes(raw)
                squares = squares + fold_lanes(raw * raw)
                scaled = (raw * before[0, :, across(part)]).astype(jnp.bfloat16)
                for start in range(0, part_width, mxu_width):
                    lhs = scaled[:, start : start + mxu_width]
                    multiply(index, acc_in, [lhs] * mxus)
                    if opening and index == tiles_in // 2 - 1:
                        pl.when(section == 0)(functools.partial(average, index % 2))
                    for mxu in range(mxus):
                        stage(index + 2, mxu)
                    index += 1
            if opening:
                row_mean[...] = popped(accs[1])[0:1] * (1.0 / mxu_width)
            mean = jnp.sum(total, axis=-1, keepdims=True) / width
            square = jnp.sum(squares, axis=-1, keepdims=True) / width
            variance = jnp.maximum(square - mean * mean, 0.0)
            scale = jnp.where(section > 0, lax.rsqrt(variance + norm_eps), 1.0)
            lower = scale * mean
            constant = folded[1] - lower * folded[0]
            projected = popped(acc_in) * scale + constant
            projected = projected.reshape(deep)
            convolved = channel[0] + projected * masked[tap_count - 1]
            for by in range(1, tap_count):
                delayed = pltpu.roll(projected, by, 1)
                convolved = convolved + delayed * masked[tap_count - 1 - by]
            convolved = convolved.reshape(flat)
            rounded = convolved.astype(jnp.bfloat16)
            lhs = [rounded[:, m * mxu_width : (m + 1) * mxu_width] for m in range(mxus)]
            early(load_out[1])
            step(index, acc_rate, lhs)
            step(index + 1, acc_input, lhs)
            index += 2
            for part in range(parts):
                gain, shift = before[0, :, across(part)], before[1, :, across(part)]
                stream = (received(part) * scale - lower) * gain + shift
                base[: count * length, across(part)] = stream
                if part == 0:
                    common = fold_lanes(stream[:, :mxu_width]) * (1.0 / mxu_width)
            rate = jnp.tanh(popped(acc_rate) + channel[1])
            fall = rate * channel[3] + channel[3]
            decay = jnp.exp2(fall * -log2_e)
            gap = jnp.tanh(fall) * (decay * decay + 1.0)
            scale_in = gap * lax.rsqrt(jnp.maximum(gap, smallest))
            half = 0.5 * convolved
            gated = jnp.tanh(popped(acc_input) + channel[2]) * half + half
            hidden = (scale_in * gated).reshape(deep)
            decay = jnp.where(position >= 1, decay.reshape(deep), 0.0)
            by = 1
            while by < length:
                hidden = decay * pltpu.roll(hidden, by, 1) + hidden
                if 2 * by < length:
                    decay = decay * pltpu.roll(decay, by, 1)
                by *= 2
            mixed = hidden.reshape(flat)
            common = common + fold_lanes(mixed * row_mean[...])
            common = jnp.sum(common, axis=-1, keepdims=True)
            mixed = mixed.astype(jnp.bfloat16)

            def project(part):
                for k in range(mxus):
                    lhs = mixed[:, k * mxu_width : (k + 1) * mxu_width]
                    multiply(index + mxus * part + k, acc_out[part], [lhs] * mxus)

            def prepare(part):
                for k in range(2):
                    for mxu in range(mxus):
                        stage(index + mxus * part + k, mxu)

            def finish(part):
                away = base[: count * length, across(part)] - common + popped(acc_out[part])
                outbox[slot, cores, :, across(part)] = away.reshape(deep).astype(jnp.bfloat16)

                @pl.when(section < last)
                def _():
                    onward(slot, first, count, part).start()

                ahead = [lead] if not opening else list(range(lead))
                behind = list(range(lead)) if not opening else [lead]
                held = range(part - 1, part + 1) if part == parts - 1 else [part]
                sends = [(core_index, part) for core_index in ahead]
                if part != parts - 2:
                    sends += [(core_index, late) for core_index in behind for late in held]
                for core_index, ready_part in sends:
                    @pl.when((section == last) & ((slot < last) | (core_index < lead)))
                    def _():
                        home(slot, core_index, ready_part).start()

            project(0)
            early(load_out[2])
            prepare(1)
            project(1)
            if opening:
                pl.when((section == 0) & (section < last))(norm_send)
            finish(0)
            early(*load_out[3:])
            for part in range(2, parts):
                prepare(part)
                project(part)
                if part < parts - 1:
                    finish(part - 1)
            prepare(parts)
            finish(parts - 2)
            finish(parts - 1)

        unit_of(0, 0, pair, accs, True)

        def one_slot(slot, carry):
            unit_of(slot, 0, pair, accs, False)
            return carry

        lax.fori_loop(1, sections, one_slot, 0)
        drain()

        @pl.when(section < last)
        def _():
            norm_onward.wait_send()
            for slot in range(sections):
                onward_all(slot).wait_send()

        @pl.when(section == last)
        def _():
            landing[...] = outbox[last, lead]
            for slot, core_index in homes:
                norm_home(slot, core_index).wait_send()
            for slot in range(last):
                homes_sent(slot, slice(0, pair)).wait_send()
            if lead:
                homes_sent(last, slice(0, lead)).wait_send()

    pairs = [accs[start : start + mxus] for start in range(0, len(accs), mxus)]

    @pl.when(leads)
    def _():
        run_section(pairs)

    @pl.when(jnp.logical_not(first_stop))
    def _():
        pltpu.make_async_remote_copy(
            src_ref=tokens_hbm.at[0, 0],
            dst_ref=inbox.at[section, core],
            send_sem=entry_sem,
            recv_sem=recv_sem.at[section, 0, 0],
            device_id=at(0, lead),
            device_id_type=MESH,
        ).wait_send()

    @pl.when(jnp.logical_not(last_stop))
    def _():
        pltpu.make_async_remote_copy(
            src_ref=norm,
            dst_ref=after,
            send_sem=entry_sem,
            recv_sem=norm_sem.at[2],
            device_id=at(0, lead),
            device_id_type=MESH,
        ).wait_recv()
        landed().wait_recv()

    raw = landing[...].astype(jnp.float32)
    mean = jnp.sum(fold_lanes(raw), axis=-1, keepdims=True) / width
    square = jnp.sum(fold_lanes(raw * raw), axis=-1, keepdims=True) / width
    variance = jnp.maximum(square - mean * mean, 0.0)
    scale = lax.rsqrt(variance + norm_eps)
    normed = (raw * scale - mean * scale) * after[0] + after[1]
    out_ref[0, 0] = normed.astype(jnp.bfloat16)


def shards(sections, pair, tokens_in, *weights):
    _, _, length, width = tokens_in.shape
    lru_width = weights[0].shape[2]
    tap_count = weights[1].shape[1]
    _, blocks, block_width, _ = weights[3].shape
    parts = width // (mxus * mxu_width)
    assert lru_width == mxus * mxu_width and mxu_width % block_width == 0
    vmem = pltpu.VMEM
    f32, bf16 = jnp.float32, jnp.bfloat16
    scoped = [
        pltpu.SemaphoreType.DMA((11 + 2 * parts,)),
        pltpu.SemaphoreType.DMA,
        pltpu.SemaphoreType.DMA((sections,)),
        pltpu.SemaphoreType.DMA((sections, pair, parts)),
        pltpu.SemaphoreType.DMA,
        pltpu.SemaphoreType.DMA((3,)),
        pltpu.SemaphoreType.DMA((sections, pair)),
        pltpu.SemaphoreType.REGULAR,
        *[
            pltpu.ACC(mxu)((pair * length, mxu_width), jnp.float32)
            for _ in range(3 + parts)
            for mxu in range(mxus)
        ],
    ]

    def kernel(*refs):
        pl.run_scoped(functools.partial(stack_kernel, sections, *refs), *scoped)

    return pl.pallas_call(
        kernel,
        out_shape=pltpu.VMEM(tokens_in.shape, tokens_in.dtype),
        in_specs=[pl.BlockSpec(memory_space=pl.ANY)] * (1 + len(weights)),
        out_specs=pl.BlockSpec(memory_space=pltpu.VMEM),
        scratch_shapes=[
            vmem((width, lru_width), bf16),
            vmem((lru_width, width), bf16),
            vmem((tap_count, lru_width), f32),
            vmem((4, 1, lru_width), f32),
            vmem((2, blocks, block_width, block_width), bf16),
            vmem((2, 1, width), f32),
            vmem((2, 1, width), f32),
            vmem((2, 1, width), f32),
            vmem((length, width), bf16),
            vmem((2, mxus, mxu_width, mxu_width), bf16),
            vmem((2, 1, lru_width), f32),
            vmem((1, lru_width), f32),
            vmem((tap_count, length, lru_width), f32),
            vmem((pair * length, width), f32),
            vmem((sections, pair, length, width), bf16),
            vmem((sections, pair, length, width), bf16),
        ],
        compiler_params=pltpu.CompilerParams(collective_id=0, has_side_effects=True),
        name="section_stack",
    )(tokens_in, *weights)


def solution(mesh):
    placed = (
        P("pp", ("fs", "tp"), None, None),
        P("pp", None, None),
        P("pp", None, None),
        P("pp", None),
        P("pp", None, None, None),
        P("pp", None),
        P("pp", None, None, None),
        P("pp", None),
        P("pp", None),
        P("pp", None, None),
        P("pp", None),
        P("pp", None),
    )
    pair = 2 if mesh.shape["tp"] % 2 == 0 else 1
    return jax.shard_map(
        functools.partial(shards, mesh.shape["pp"], pair),
        mesh=mesh,
        in_specs=placed,
        out_specs=P("pp", ("fs", "tp"), None, None),
        check_vma=False,
    )
```

```python
import functools

import jax
import jax.numpy as jnp
from jax import lax
from jax.experimental import pallas as pl
from jax.experimental.pallas import tpu as pltpu
from jax.sharding import PartitionSpec as P

decay_scale = 8.0
norm_eps = 1e-05
mxu_width = 256
mxus = 2
lanes = 128
smallest = 1e-30
log2_e = 1.4426950408889634
MESH = pl.DeviceIdType.MESH


def fold_lanes(x):
    total = x[:, :lanes]
    for start in range(lanes, x.shape[1], lanes):
        total = total + x[:, start : start + lanes]
    return total


def stack_kernel(
    sections,
    tokens_hbm,
    w_in_hbm,
    taps_hbm,
    cbias_hbm,
    grate_hbm,
    brate_hbm,
    ginput_hbm,
    binput_hbm,
    dparam_hbm,
    w_out_hbm,
    gain_hbm,
    shift_hbm,
    out_ref,
    w_in,
    w_out,
    taps,
    channel,
    gates,
    norm,
    before,
    after,
    landing,
    maps,
    folded,
    row_mean,
    masked,
    base,
    inbox,
    outbox,
    load_sem,
    entry_sem,
    send_sem,
    recv_sem,
    final_sem,
    norm_sem,
    home_sem,
    ready_sem,
    *accs,
):
    section = lax.axis_index("pp")
    column = lax.axis_index("tp")
    last = sections - 1
    pair, length = inbox.shape[1:3]
    rows = pair * length
    width, lru_width = w_in.shape
    parts = recv_sem.shape[2]
    part_width = width // parts
    tiles_in = width // mxu_width
    core = lax.rem(column, pair)
    lead = pair - 1
    leads = core == lead
    first_stop = leads & (section == 0)
    last_stop = leads & (section == last)

    columns = [column - core + core_index for core_index in range(pair)]
    onward_stop = jnp.minimum(section + 1, last)

    def at(stop, core_index):
        known = isinstance(core_index, int)
        return {"pp": stop, "tp": columns[core_index] if known else columns[0] + core_index}

    def across(part):
        return slice(part * part_width, (part + 1) * part_width)

    barrier = pltpu.get_barrier_semaphore()

    def tell(stop, core_index):
        pl.semaphore_signal(
            barrier, inc=1, device_id=at(stop, core_index), device_id_type=MESH
        )

    def load(src, dst, index):
        return pltpu.make_async_copy(src, dst, load_sem.at[index])

    own = load(tokens_hbm.at[0, 0], inbox.at[0, lead], 0)
    small = [
        load(grate_hbm.at[0], gates.at[0], 1),
        load(ginput_hbm.at[0], gates.at[1], 2),
        load(taps_hbm.at[0], taps, 3),
        load(cbias_hbm, channel.at[0], 4),
        load(brate_hbm, channel.at[1], 5),
        load(binput_hbm, channel.at[2], 6),
        load(dparam_hbm, channel.at[3], 7),
        load(gain_hbm, norm.at[0], 8),
        load(shift_hbm, norm.at[1], 9),
    ]
    load_in = [
        load(w_in_hbm.at[0, across(part)], w_in.at[across(part)], 10 + part)
        for part in range(parts)
    ]
    out_cols = [slice(0, mxu_width), slice(mxu_width, part_width)]
    out_cols += [across(part) for part in range(1, parts)]
    load_out = [
        load(w_out_hbm.at[0, :, cols], w_out.at[:, cols], 10 + parts + index)
        for index, cols in enumerate(out_cols)
    ]

    @pl.when(first_stop)
    def _():
        for stop in reversed(range(sections)):
            for core_index in range(pair):
                if (stop, core_index) != (0, lead):
                    tell(stop, core_index)

    @pl.when(jnp.logical_not(first_stop | last_stop))
    def _():
        tell(last, lead)

    @pl.when(leads & (section > 0) & (section + 1 < last))
    def _():
        tell(section + 1, lead)

    heard = jnp.where(
        last_stop, sections * pair - 1, jnp.where(leads & (section > 1), 2, 1)
    ).astype(jnp.int32)

    def entry(part):
        return pltpu.make_async_remote_copy(
            src_ref=tokens_hbm.at[0, 0, :, across(part)],
            dst_ref=inbox.at[section, core, :, across(part)],
            send_sem=entry_sem,
            recv_sem=recv_sem.at[section, 0, part],
            device_id=at(0, lead),
            device_id_type=MESH,
        )

    @pl.when(jnp.logical_not(first_stop))
    def _():
        pl.semaphore_wait(barrier, heard)
        for part in range(parts):
            entry(part).start()

    @pl.when(first_stop)
    def _():
        own.start()

    @pl.when(leads & (section > 0))
    def _():
        pl.semaphore_signal(
            ready_sem, inc=1, device_id=at(section - 1, lead), device_id_type=MESH
        )

    @pl.when(leads)
    def _():
        for copy in small + load_in[:2] + load_out[:1] + load_in[2:] + load_out[1:]:
            copy.start()

    def onward(slot, first, count, part):
        cores = pl.ds(first, count)
        return pltpu.make_async_remote_copy(
            src_ref=outbox.at[slot, cores, :, across(part)],
            dst_ref=inbox.at[slot, cores, :, across(part)],
            send_sem=send_sem.at[slot],
            recv_sem=recv_sem.at[slot, first, part],
            device_id=at(onward_stop, lead),
            device_id_type=MESH,
        )

    def onward_all(slot):
        return pltpu.make_async_remote_copy(
            src_ref=outbox.at[slot],
            dst_ref=inbox.at[slot],
            send_sem=send_sem.at[slot],
            recv_sem=recv_sem.at[slot, 0, 0],
            device_id=at(onward_stop, lead),
            device_id_type=MESH,
        )

    def home(slot, core_index, part):
        return pltpu.make_async_remote_copy(
            src_ref=outbox.at[slot, core_index, :, across(part)],
            dst_ref=landing.at[:, across(part)],
            send_sem=send_sem.at[slot],
            recv_sem=final_sem,
            device_id=at(slot, core_index),
            device_id_type=MESH,
        )

    def landed():
        return pltpu.make_async_remote_copy(
            src_ref=landing,
            dst_ref=landing,
            send_sem=entry_sem,
            recv_sem=final_sem,
            device_id=at(0, lead),
            device_id_type=MESH,
        )

    def norm_home(slot, core_index):
        return pltpu.make_async_remote_copy(
            src_ref=norm,
            dst_ref=after,
            send_sem=home_sem.at[slot, core_index],
            recv_sem=norm_sem.at[2],
            device_id=at(slot, core_index),
            device_id_type=MESH,
        )

    homes = [
        (slot, core_index)
        for slot in range(sections)
        for core_index in reversed(range(pair))
        if (slot, core_index) != (last, lead)
    ]

    def homes_sent(slot, cores):
        return pltpu.make_async_remote_copy(
            src_ref=outbox.at[slot, cores],
            dst_ref=inbox.at[slot, cores],
            send_sem=send_sem.at[slot],
            recv_sem=final_sem,
            device_id=at(slot, lead),
            device_id_type=MESH,
        )

    norm_onward = pltpu.make_async_remote_copy(
        src_ref=norm,
        dst_ref=before,
        send_sem=norm_sem.at[0],
        recv_sem=norm_sem.at[1],
        device_id=at(onward_stop, lead),
        device_id_type=MESH,
    )

    def tile(ref, row, col):
        return ref[
            row * mxu_width : (row + 1) * mxu_width,
            col * mxu_width : (col + 1) * mxu_width,
        ]

    def unit(index, mxu):
        index = index % (tiles_in + 2 + mxus * parts)
        if index < tiles_in:
            return tile(w_in, index, mxu)
        index -= tiles_in
        if index < 2:
            return maps[index, mxu]
        index -= 2
        return tile(w_out, index % mxus, (index // mxus) * mxus + mxu)

    def stage(index, mxu):
        pltpu.matmul_push_rhs(unit(index, mxu), staging_register=index % 2, mxu_index=mxu)

    def multiply(index, accs, lhs):
        for mxu in range(mxus):
            pltpu.matmul_acc_lhs(accs[mxu], lhs[mxu], load_staged_rhs=index % 2)

    def step(index, accs, lhs):
        multiply(index, accs, lhs)
        for mxu in range(mxus):
            stage(index + 2, mxu)

    def popped(accs):
        return jnp.concatenate([pltpu.matmul_pop(acc) for acc in accs], axis=1)

    def run_section(accs):
        def drain():
            nothing = jnp.zeros((rows, mxu_width), jnp.float32)
            for mxu in range(mxus):
                for register in range(2):
                    pltpu.matmul_acc_lhs(accs[0][mxu], nothing, load_staged_rhs=register)
            popped(accs[0])

        drain()
        for acc in accs[1:]:
            popped(acc)
        _, blocks, block_width, _ = gates.shape
        group = mxu_width // block_width
        maps[...] = jnp.zeros_like(maps)
        for copy in small:
            copy.wait()

        def norm_send():
            pl.semaphore_wait(ready_sem, 1)
            norm_onward.start()

        pl.when((section > 0) & (section < last))(norm_send)

        for gate in range(2):
            for block in range(blocks):
                to = (block % group) * block_width
                maps[gate, block // group, to : to + block_width, to : to + block_width] = (
                    gates[gate, block] * 0.5
                )
        minus_decay = -channel[3]
        softplus = jnp.maximum(minus_decay, 0.0) + jnp.log1p(jnp.exp(-jnp.abs(minus_decay)))
        channel[3] = 0.5 * decay_scale * softplus
        channel[1] = 0.5 * channel[1]
        channel[2] = 0.5 * channel[2]
        position = lax.broadcasted_iota(jnp.int32, (length, lru_width), 0)
        tap_count = taps.shape[0]
        for tap in range(tap_count):
            masked[tap] = jnp.where(position >= tap_count - 1 - tap, taps[tap : tap + 1], 0.0)

        def norm_rows(index):
            cols = slice(index * mxu_width, (index + 1) * mxu_width)
            which = lax.broadcasted_iota(jnp.int32, (rows, mxu_width), 0)
            lhs = jnp.zeros((rows, mxu_width), jnp.float32)
            for vector in range(2):
                value = before[vector, :, cols]
                high = value.astype(jnp.bfloat16).astype(jnp.float32)
                lhs = jnp.where(which == 2 * vector, high, lhs)
                lhs = jnp.where(which == 2 * vector + 1, value - high, lhs)
            return lhs.astype(jnp.bfloat16)

        def average(register):
            load_out[0].wait()
            ones = jnp.ones((rows, mxu_width), jnp.float32)
            for mxu in range(mxus):
                pltpu.matmul_push_rhs(
                    tile(w_out, mxu, 0),
                    staging_register=register,
                    mxu_index=mxu,
                    transpose=True,
                )
            multiply(register, accs[1], [ones] * mxus)

        @pl.when(first_stop)
        def _():
            own.wait()
            load_in[0].wait()
            folded[...] = jnp.zeros_like(folded)
            before[0] = jnp.ones_like(before[0])
            before[1] = jnp.zeros_like(before[1])

        @pl.when(section > 0)
        def _():
            average(0)
            for copy in load_in + load_out[1:]:
                copy.wait()
            norm_onward.wait_recv()
            for k in range(tiles_in):
                for mxu in range(mxus):
                    stage(k, mxu)
                multiply(k, accs[0], [norm_rows(k)] * mxus)
            result = popped(accs[0])
            folded[0] = result[0:1] + result[1:2]
            folded[1] = result[2:3] + result[3:4]

        for mxu in range(mxus):
            stage(0, mxu)
            stage(1, mxu)
        @pl.when(section == last)
        def _():
            after[...] = norm[...]
            for slot, core_index in homes:
                norm_home(slot, core_index).start()

        def unit_of(slot, first, count, accs, opening):
            acc_in, acc_rate, acc_input, *acc_out = accs
            flat, deep = (count * length, -1), (count, length, -1)
            cores = pl.ds(first, count)

            def received(part):
                raw = inbox[slot, cores, :, across(part)]
                return raw.astype(jnp.float32).reshape(flat)

            def early(*copies):
                if opening:
                    @pl.when(section == 0)
                    def _():
                        for copy in copies:
                            copy.wait()

            total = jnp.zeros((count * length, lanes), jnp.float32)
            squares = jnp.zeros((count * length, lanes), jnp.float32)
            index = 0
            for part in range(parts):
                if opening:
                    @pl.when(section > 0)
                    def _():
                        onward(slot, first, count, part).wait_recv()

                    for other in range(lead):
                        @pl.when(section == 0)
                        def _():
                            onward(slot, other, 1, part).wait_recv()

                    early(*load_in[part + 1 : part + 2])
                else:
                    onward(slot, first, count, part).wait_recv()
                raw = received(part)
                total = total + fold_lanes(raw)
                squares = squares + fold_lanes(raw * raw)
                scaled = (raw * before[0, :, across(part)]).astype(jnp.bfloat16)
                for start in range(0, part_width, mxu_width):
                    lhs = scaled[:, start : start + mxu_width]
                    multiply(index, acc_in, [lhs] * mxus)
                    if opening and index == tiles_in // 2 - 1:
                        pl.when(section == 0)(functools.partial(average, index % 2))
                    for mxu in range(mxus):
                        stage(index + 2, mxu)
                    index += 1
            if opening:
                row_mean[...] = popped(accs[1])[0:1] * (1.0 / mxu_width)
            mean = jnp.sum(total, axis=-1, keepdims=True) / width
            square = jnp.sum(squares, axis=-1, keepdims=True) / width
            variance = jnp.maximum(square - mean * mean, 0.0)
            scale = jnp.where(section > 0, lax.rsqrt(variance + norm_eps), 1.0)
            lower = scale * mean
            constant = folded[1] - lower * folded[0]
            projected = popped(acc_in) * scale + constant
            projected = projected.reshape(deep)
            convolved = channel[0] + projected * masked[tap_count - 1]
            for by in range(1, tap_count):
                delayed = pltpu.roll(projected, by, 1)
                convolved = convolved + delayed * masked[tap_count - 1 - by]
            convolved = convolved.reshape(flat)
            rounded = convolved.astype(jnp.bfloat16)
            lhs = [rounded[:, m * mxu_width : (m + 1) * mxu_width] for m in range(mxus)]
            early(load_out[1])
            step(index, acc_rate, lhs)
            step(index + 1, acc_input, lhs)
            index += 2
            for part in range(parts):
                gain, shift = before[0, :, across(part)], before[1, :, across(part)]
                stream = (received(part) * scale - lower) * gain + shift
                base[: count * length, across(part)] = stream
                if part == 0:
                    common = fold_lanes(stream[:, :mxu_width]) * (1.0 / mxu_width)
            rate = jnp.tanh(popped(acc_rate) + channel[1])
            fall = rate * channel[3] + channel[3]
            decay = jnp.exp2(fall * -log2_e)
            gap = jnp.tanh(fall) * (decay * decay + 1.0)
            scale_in = gap * lax.rsqrt(jnp.maximum(gap, smallest))
            half = 0.5 * convolved
            gated = jnp.tanh(popped(acc_input) + channel[2]) * half + half
            hidden = (scale_in * gated).reshape(deep)
            decay = jnp.where(position >= 1, decay.reshape(deep), 0.0)
            by = 1
            while by < length:
                hidden = decay * pltpu.roll(hidden, by, 1) + hidden
                if 2 * by < length:
                    decay = decay * pltpu.roll(decay, by, 1)
                by *= 2
            mixed = hidden.reshape(flat)
            common = common + fold_lanes(mixed * row_mean[...])
            common = jnp.sum(common, axis=-1, keepdims=True)
            mixed = mixed.astype(jnp.bfloat16)

            def project(part):
                for k in range(mxus):
                    lhs = mixed[:, k * mxu_width : (k + 1) * mxu_width]
                    multiply(index + mxus * part + k, acc_out[part], [lhs] * mxus)

            def prepare(part):
                for k in range(2):
                    for mxu in range(mxus):
                        stage(index + mxus * part + k, mxu)

            def finish(part):
                away = base[: count * length, across(part)] - common + popped(acc_out[part])
                outbox[slot, cores, :, across(part)] = away.reshape(deep).astype(jnp.bfloat16)

                @pl.when(section < last)
                def _():
                    onward(slot, first, count, part).start()

                ahead = [lead] if not opening else list(range(lead))
                behind = list(range(lead)) if not opening else [lead]
                held = range(part - 1, part + 1) if part == parts - 1 else [part]
                sends = [(core_index, part) for core_index in ahead]
                if part != parts - 2:
                    sends += [(core_index, late) for core_index in behind for late in held]
                for core_index, ready_part in sends:
                    @pl.when((section == last) & ((slot < last) | (core_index < lead)))
                    def _():
                        home(slot, core_index, ready_part).start()

            project(0)
            early(load_out[2])
            prepare(1)
            project(1)
            if opening:
                pl.when((section == 0) & (section < last))(norm_send)
            finish(0)
            early(*load_out[3:])
            for part in range(2, parts):
                prepare(part)
                project(part)
                if part < parts - 1:
                    finish(part - 1)
            prepare(parts)
            finish(parts - 2)
            finish(parts - 1)

        unit_of(0, 0, pair, accs, True)

        def one_slot(slot, carry):
            unit_of(slot, 0, pair, accs, False)
            return carry

        lax.fori_loop(1, sections, one_slot, 0)
        drain()

        @pl.when(section < last)
        def _():
            norm_onward.wait_send()
            for slot in range(sections):
                onward_all(slot).wait_send()

        @pl.when(section == last)
        def _():
            landing[...] = outbox[last, lead]
            for slot, core_index in homes:
                norm_home(slot, core_index).wait_send()
            for slot in range(last):
                homes_sent(slot, slice(0, pair)).wait_send()
            if lead:
                homes_sent(last, slice(0, lead)).wait_send()

    pairs = [accs[start : start + mxus] for start in range(0, len(accs), mxus)]

    @pl.when(leads)
    def _():
        run_section(pairs)

    @pl.when(jnp.logical_not(first_stop))
    def _():
        pltpu.make_async_remote_copy(
            src_ref=tokens_hbm.at[0, 0],
            dst_ref=inbox.at[section, core],
            send_sem=entry_sem,
            recv_sem=recv_sem.at[section, 0, 0],
            device_id=at(0, lead),
            device_id_type=MESH,
        ).wait_send()

    @pl.when(jnp.logical_not(last_stop))
    def _():
        pltpu.make_async_remote_copy(
            src_ref=norm,
            dst_ref=after,
            send_sem=entry_sem,
            recv_sem=norm_sem.at[2],
            device_id=at(0, lead),
            device_id_type=MESH,
        ).wait_recv()
        landed().wait_recv()

    raw = landing[...].astype(jnp.float32)
    mean = jnp.sum(fold_lanes(raw), axis=-1, keepdims=True) / width
    square = jnp.sum(fold_lanes(raw * raw), axis=-1, keepdims=True) / width
    variance = jnp.maximum(square - mean * mean, 0.0)
    scale = lax.rsqrt(variance + norm_eps)
    normed = (raw * scale - mean * scale) * after[0] + after[1]
    out_ref[0, 0] = normed.astype(jnp.bfloat16)


def shards(sections, pair, tokens_in, *weights):
    _, _, length, width = tokens_in.shape
    lru_width = weights[0].shape[2]
    tap_count = weights[1].shape[1]
    _, blocks, block_width, _ = weights[3].shape
    parts = width // (mxus * mxu_width)
    assert lru_width == mxus * mxu_width and mxu_width % block_width == 0
    vmem = pltpu.VMEM
    f32, bf16 = jnp.float32, jnp.bfloat16
    scoped = [
        pltpu.SemaphoreType.DMA((11 + 2 * parts,)),
        pltpu.SemaphoreType.DMA,
        pltpu.SemaphoreType.DMA((sections,)),
        pltpu.SemaphoreType.DMA((sections, pair, parts)),
        pltpu.SemaphoreType.DMA,
        pltpu.SemaphoreType.DMA((3,)),
        pltpu.SemaphoreType.DMA((sections, pair)),
        pltpu.SemaphoreType.REGULAR,
        *[
            pltpu.ACC(mxu)((pair * length, mxu_width), jnp.float32)
            for _ in range(3 + parts)
            for mxu in range(mxus)
        ],
    ]

    def kernel(*refs):
        pl.run_scoped(functools.partial(stack_kernel, sections, *refs), *scoped)

    return pl.pallas_call(
        kernel,
        out_shape=pltpu.VMEM(tokens_in.shape, tokens_in.dtype),
        in_specs=[pl.BlockSpec(memory_space=pl.ANY)] * (1 + len(weights)),
        out_specs=pl.BlockSpec(memory_space=pltpu.VMEM),
        scratch_shapes=[
            vmem((width, lru_width), bf16),
            vmem((lru_width, width), bf16),
            vmem((tap_count, lru_width), f32),
            vmem((4, 1, lru_width), f32),
            vmem((2, blocks, block_width, block_width), bf16),
            vmem((2, 1, width), f32),
            vmem((2, 1, width), f32),
            vmem((2, 1, width), f32),
            vmem((length, width), bf16),
            vmem((2, mxus, mxu_width, mxu_width), bf16),
            vmem((2, 1, lru_width), f32),
            vmem((1, lru_width), f32),
            vmem((tap_count, length, lru_width), f32),
            vmem((pair * length, width), f32),
            vmem((sections, pair, length, width), bf16),
            vmem((sections, pair, length, width), bf16),
        ],
        compiler_params=pltpu.CompilerParams(collective_id=0, has_side_effects=True),
        name="section_stack",
    )(tokens_in, *weights)


def solution(mesh):
    placed = (
        P("pp", ("fs", "tp"), None, None),
        P("pp", None, None),
        P("pp", None, None),
        P("pp", None),
        P("pp", None, None, None),
        P("pp", None),
        P("pp", None, None, None),
        P("pp", None),
        P("pp", None),
        P("pp", None, None),
        P("pp", None),
        P("pp", None),
    )
    pair = 2 if mesh.shape["tp"] % 2 == 0 else 1
    return jax.shard_map(
        functools.partial(shards, mesh.shape["pp"], pair),
        mesh=mesh,
        in_specs=placed,
        out_specs=P("pp", ("fs", "tp"), None, None),
        check_vma=False,
    )
```
